256 devices in a mesh: fs: 32 (over z, x), tp: 8 (over y, core).
Axes of the slice: x: 4, y: 4, z: 8, core: 2. Of those that a mesh axis runs over, the one named last changes fastest.
Arguments:
- normed_inputs: bfloat16 [196608, 2048], P(('fs', 'tp')), may hold values from -24 to 24
- query_cotangent: bfloat16 [196608, 1024], P(('fs', 'tp')), may hold values from -6 to 6
- head_outputs: bfloat16 [196608, 1024], P(('fs', 'tp')), may hold values from -24 to 24
- output_cotangent: bfloat16 [196608, 2048], P(('fs', 'tp')), may hold values from -6 to 6
- query_weight: float32 [2048, 1024], P('fs', 'tp'), may hold values from -0.125 to 0.125
- out_weight: float32 [1024, 2048], P('fs', 'tp'), may hold values from -0.1875 to 0.1875
- query_basis: bfloat16 [2048, 512], P('fs'), may hold values from -0.125 to 0.125
- out_basis: bfloat16 [1024, 512], P('fs'), may hold values from -0.1875 to 0.1875
- query_mean: float32 [512, 1024], P('fs', 'tp'), may hold values from -6 to 6
- query_square: float32 [512, 1024], P('fs', 'tp'), may hold values from 0.5 to 2
- out_mean: float32 [512, 2048], P('fs', 'tp'), may hold values from -6 to 6
- out_square: float32 [512, 2048], P('fs', 'tp'), may hold values from 0.5 to 2
Outputs:
- query_mean_new: float32 [512, 1024], P('fs', 'tp')
- query_square_new: float32 [512, 1024], P('fs', 'tp')
- query_step: float32 [2048, 1024], P('fs', 'tp')
- query_weight_new: float32 [2048, 1024], P('fs', 'tp')
- query_copy: bfloat16 [2048, 1024], P(None, 'tp')
- out_mean_new: float32 [512, 2048], P('fs', 'tp')
- out_square_new: float32 [512, 2048], P('fs', 'tp')
- out_step: float32 [1024, 2048], P('fs', 'tp')
- out_weight_new: float32 [1024, 2048], P('fs', 'tp')
- out_copy: bfloat16 [1024, 2048], P(None, 'tp')
The draws below stay inside these ranges and needn't reach their ends.
All inputs are finite; a program needn't handle non-finite values.
Results may differ from the reference program's by a relative error of at most 0.009.
Values may be sent and summed in bfloat16 or wider, within the bound.
A program may use at most 64 MiB of HBM per device.

```python
import math
import jax
import jax.numpy as jnp
from jax import lax

D = 2048
QW = 1024
RANK = 512
TOK_DEV = 768
TOKENS = 196608


def strengthened(array, stream_key, source, target, blocks, factor):
    def block_of(position):
        return (jnp.arange(array.shape[position]) // (array.shape[position] // blocks)).reshape((-1,) + (1,) * (array.ndim - 1 - position))

    one_side = jax.random.permutation(stream_key, blocks)[block_of(target)]
    second = (block_of(target) + blocks // 2) % blocks
    return jnp.where((block_of(source) == one_side) | (block_of(source) == second), factor * array, array)


def block_scale(own_key, extent, shards, least, top_value):
    loudness, own = 1.0, jax.random.fold_in(own_key, 6)
    for axis_at, shards_of in shards:
        heights = jnp.exp(jax.random.uniform(jax.random.fold_in(own, axis_at), (shards_of,), jnp.float32, least / len(shards), top_value / len(shards)))
        loudness = loudness * jnp.repeat(heights, extent[axis_at] // shards_of).reshape([-1 if axis == axis_at else 1 for axis in range(len(extent))])
    return loudness


def normal_values(own_key, extent, deviation, reach, cuts=(), kind=jnp.bfloat16):
    loudness = block_scale(own_key, extent, cuts, -0.22, 0.18) if cuts else 1.0
    result = jax.random.normal(own_key, extent, jnp.float32) * deviation * loudness
    return jnp.minimum(jnp.maximum(result, -reach), reach).astype(kind)


def heavy_noise(stream_key, dims, scale, limit, shards, heavy, dtype=jnp.bfloat16):
    result = scale * jax.random.normal(stream_key, dims, jnp.float32)
    if shards:
        result = result * block_scale(stream_key, dims, shards, -0.22, 0.18)
    return jnp.clip(strengthened(result, jax.random.fold_in(stream_key, 3), *heavy), -limit, limit).astype(dtype)


def setup_inputs(seed: int = 0) -> dict:
    seeds = jax.random.split(jax.random.key(seed), 13)
    normed_inputs = heavy_noise(seeds[0], (TOKENS, D), 1.0, 24.0, ((0, 256),), (0, 1, 256, 6.0))
    query_cotangent = normal_values(seeds[1], (TOKENS, QW), 1.0, 6.0, ((0, 256),))
    head_outputs = heavy_noise(seeds[2], (TOKENS, QW), 1.0, 24.0, ((0, 256),), (0, 1, 256, 6.0))
    output_cotangent = normal_values(seeds[3], (TOKENS, D), 1.0, 6.0, ((0, 256),))
    query_weight = normal_values(seeds[4], (D, QW), D ** -0.5, 0.125, ((0, 32), (1, 8)), jnp.float32)
    out_weight = normal_values(seeds[5], (QW, D), QW ** -0.5, 0.1875, ((0, 32), (1, 8)), jnp.float32)
    query_basis = normal_values(seeds[6], (D, RANK), D ** -0.5, 0.125, ((0, 32),))
    out_basis = normal_values(seeds[7], (QW, RANK), QW ** -0.5, 0.1875, ((0, 32),))
    query_mean = normal_values(seeds[8], (RANK, QW), 1.0, 6.0, ((0, 32), (1, 8)), jnp.float32)
    query_square = jnp.clip(jnp.exp(math.log(2.0) - 1.3862944 * jax.random.uniform(seeds[9], (RANK, QW), jnp.float32) ** block_scale(seeds[9], (RANK, QW), ((0, 32), (1, 8)), -0.2, 0.2)), 0.5, 2.0)
    out_mean = normal_values(seeds[10], (RANK, D), 1.0, 6.0, ((0, 32), (1, 8)), jnp.float32)
    out_square = jnp.clip(jnp.exp(math.log(2.0) - 1.3862944 * jax.random.uniform(seeds[11], (RANK, D), jnp.float32) ** block_scale(seeds[11], (RANK, D), ((0, 32), (1, 8)), -0.2, 0.2)), 0.5, 2.0)
    return dict(normed_inputs=normed_inputs, query_cotangent=query_cotangent, head_outputs=head_outputs, output_cotangent=output_cotangent, query_weight=query_weight, out_weight=out_weight, query_basis=query_basis, out_basis=out_basis, query_mean=query_mean, query_square=query_square, out_mean=out_mean, out_square=out_square)


def update_matrix(grad, basis, mean, square, weight):
    wide_basis = basis.astype(jnp.float32)
    reduced = jnp.dot(wide_basis.T, grad, precision=lax.Precision.HIGHEST)
    mean_new = 0.8 * mean + 0.2 * reduced
    square_new = 0.9 * square + 0.1 * reduced * reduced
    direction = mean_new / (jnp.sqrt(square_new) + 1e-08)
    full = jnp.dot(wide_basis, direction, precision=lax.Precision.HIGHEST)
    step = full * lax.rsqrt(lax.optimization_barrier(jnp.mean(full * full, axis=0)) + 0.05)
    weight_new = weight - 0.01 * step
    return (mean_new, square_new, step, weight_new, weight_new.astype(jnp.bfloat16))

def reference(normed_inputs, query_cotangent, head_outputs, output_cotangent, query_weight, out_weight, query_basis, out_basis, query_mean, query_square, out_mean, out_square):
    blocks = TOKENS // TOK_DEV
    inputs_blocks = normed_inputs.reshape(blocks, TOK_DEV, D)
    query_blocks = query_cotangent.reshape(blocks, TOK_DEV, QW)
    heads_blocks = head_outputs.reshape(blocks, TOK_DEV, QW)
    output_blocks = output_cotangent.reshape(blocks, TOK_DEV, D)

    def accumulate(totals, pieces):
        inputs_part, query_part, heads_part, output_part = pieces
        query_total = totals[0] + jnp.dot(inputs_part.astype(jnp.float32).T, query_part.astype(jnp.float32), precision=lax.Precision.HIGHEST)
        out_total = totals[1] + jnp.dot(heads_part.astype(jnp.float32).T, output_part.astype(jnp.float32), precision=lax.Precision.HIGHEST)
        return ((query_total, out_total), None)
    start_totals = (jnp.zeros((D, QW), jnp.float32), jnp.zeros((QW, D), jnp.float32))
    totals, unused = lax.scan(accumulate, start_totals, (inputs_blocks, query_blocks, heads_blocks, output_blocks))
    token_scale = TOKENS ** (-0.5)
    query_grad = totals[0] * token_scale
    out_grad = totals[1] * token_scale
    query_results = update_matrix(query_grad, query_basis, query_mean, query_square, query_weight)
    out_results = update_matrix(out_grad, out_basis, out_mean, out_square, out_weight)
    return (query_results[0], query_results[1], query_results[2], query_results[3], query_results[4], out_results[0], out_results[1], out_results[2], out_results[3], out_results[4])
```

```python
import functools

import jax
import jax.numpy as jnp
from jax import lax
from jax.experimental import pallas as pl
from jax.experimental.pallas import tpu as pltpu
from jax.sharding import Mesh
from jax.sharding import PartitionSpec as P

FS = ("z", "x")
FS_TP = ("z", "x", "y", "c")
TP = ("y", "c")
MESH = pl.DeviceIdType.MESH
F32 = jnp.float32
BF16 = jnp.bfloat16
LIMIT = 60 * 1024 * 1024


def nearest_first(n):
    return sorted(range(1, n), key=lambda d: (min(d, n - d), d))


def dot(a, b):
    return jnp.dot(a, b, preferred_element_type=F32)


def exchange(sizes, *refs):
    Z, X, Y, token_scale = sizes
    (xin, qcin, hin, ocin, qbin, obin, qw, ow, qm, qs, om, os_,
     qb_out, ob_out, wg_out, dg_out, qm_out, qs_out, om_out, os_out,
     QB, OB, WG, DG, vx, vqc, vh, voc, lot, lqt,
     pso, pro, yso, yro, xso, xro, zso, zro,
     psq, prq, mq, xsq, xrq, zsq, zrq, ysq, yrq,
     loc, snd, rzo, rxo, rzq, rxq, rzw, rzg, one,
     s_pro, s_yro, s_xro, s_zro, s_prq, s_xrq, s_zrq, s_yrq) = refs
    z, x, y, c = (lax.axis_index(name) for name in ("z", "x", "y", "c"))
    other = 1 - c
    fs = z * X + x
    rank_rows, q_cols = qm.shape
    o_cols = om.shape[1]
    q_rows, o_rows = qw.shape[0], ow.shape[0]

    def local(src, dst, number):
        copy = pltpu.make_async_copy(src, dst, loc.at[number])
        copy.start()
        return copy

    def to(src, dst, send, recv, **where):
        copy = pltpu.make_async_remote_copy(
            src_ref=src, dst_ref=dst, send_sem=send, recv_sem=recv, device_id=where, device_id_type=MESH
        )
        copy.start()

    def received(ref, recv):
        pltpu.make_async_remote_copy(
            src_ref=ref, dst_ref=ref, send_sem=snd.at[0], recv_sem=recv, device_id={"c": other}, device_id_type=MESH
        ).wait_recv()

    def sent(ref, send):
        pltpu.make_async_remote_copy(
            src_ref=ref, dst_ref=ref, send_sem=send, recv_sem=one.at[0], device_id={"c": other}, device_id_type=MESH
        ).wait_send()

    def up(at, d, n):
        return lax.rem(at + d, n)

    def down(at, d, n):
        return lax.rem(at + (n - d), n)

    zs, xs, ys = nearest_first(Z), nearest_first(X), nearest_first(Y)

    own_ob = local(obin, OB.at[fs], 0)
    own_qb = local(qbin, QB.at[fs], 1)
    get_h = local(hin, vh, 2)
    get_oc = local(ocin, voc, 3)
    get_x = local(xin, vx, 4)
    get_qc = local(qcin, vqc, 5)
    WG[fs, 0:q_rows, :] = qw[...].astype(BF16)
    for half in range(o_cols // q_cols):
        WG[fs, q_rows + half * o_rows : q_rows + (half + 1) * o_rows, :] = ow[
            :, half * q_cols : (half + 1) * q_cols
        ].astype(BF16)

    barrier = pltpu.get_barrier_semaphore()
    for d in zs:
        pl.semaphore_signal(barrier, inc=1, device_id={"z": up(z, d, Z)}, device_id_type=MESH)
    for d in xs:
        pl.semaphore_signal(barrier, inc=1, device_id={"x": up(x, d, X)}, device_id_type=MESH)
    for d in ys:
        pl.semaphore_signal(barrier, inc=1, device_id={"y": up(y, d, Y)}, device_id_type=MESH)
    pl.semaphore_signal(barrier, inc=1, device_id={"c": other}, device_id_type=MESH)
    pl.semaphore_wait(barrier, len(zs) + len(xs) + len(ys) + 1)

    def send_z(ref, index, send, rz):
        for d in zs:
            to(ref.at[index], ref.at[index], send, rz.at[d - 1], z=up(z, d, Z))

    def send_x(ref, index, send, rx_of):
        for d in xs:
            to(ref.at[index], ref.at[index], send, rx_of(d), x=up(x, d, X))

    def basis_from_z(B, d, send, rz, rx, rd):
        block = down(z, d, Z) * X + x
        received(B.at[block, c], rz.at[d - 1])
        send_x(B, (block, c), send, lambda e: rx.at[d, e - 1])
        to(B.at[block, c], B.at[block, c], send, rd, c=other)

    def basis_from_x(B, send, rx, rd):
        for d in [0] + zs:
            for e in xs:
                block = down(z, d, Z) * X + down(x, e, X)
                received(B.at[block, c], rx.at[d, e - 1])
                to(B.at[block, c], B.at[block, c], send, rd, c=other)

    def basis_whole(B, rd):
        received(B.at[pl.ds(0, Z * X - 1), 0], rd)

    own_ob.wait()
    send_z(OB, (fs, c), snd.at[0], rzo)
    send_x(OB, (fs, c), snd.at[0], lambda e: rxo.at[0, e - 1])
    own_qb.wait()
    send_z(QB, (fs, c), snd.at[1], rzq)
    for d in zs:
        basis_from_z(OB, d, snd.at[0], rzo, rxo, one.at[1])
    send_x(QB, (fs, c), snd.at[1], lambda e: rxq.at[0, e - 1])
    early = zs[: len(zs) // 2 + 1]
    for d in early:
        basis_from_z(QB, d, snd.at[1], rzq, rxq, one.at[2])
    basis_from_x(OB, snd.at[0], rxo, one.at[1])
    basis_whole(OB, one.at[1])
    put_ob = local(OB, ob_out, 6)

    def left(tokens, B, into, tile):
        width = B.shape[3]
        for at in range(0, width, tile):
            rows = B[:, :, :, at : at + tile].reshape(-1, tile)
            into[at : at + tile, :] = dot(tokens[...], rows).astype(BF16).T

    get_h.wait()
    left(vh, OB, lot, 256 if OB.shape[3] % 256 == 0 else OB.shape[3])
    for d in zs[len(early) :]:
        basis_from_z(QB, d, snd.at[1], rzq, rxq, one.at[2])
    get_oc.wait()
    for yy in range(Y):
        at = pl.multiple_of((yy * 2 + other) * o_cols, o_cols)
        pso[yy] = dot(lot[...], voc[:, pl.ds(at, o_cols)]).astype(BF16)
        to(pso.at[yy], pro.at[yy], snd.at[2], s_pro.at[yy], c=other)
    for d in ys + [0]:
        yy = up(y, d, Y)
        at = pl.multiple_of((yy * 2 + c) * o_cols, o_cols)
        mine = dot(lot[...], voc[:, pl.ds(at, o_cols)])
        received(pro.at[yy], s_pro.at[yy])
        yso[d] = (mine + pro[yy].astype(F32)).astype(BF16)
        if d:
            to(yso.at[d], yro.at[d - 1], snd.at[3], s_yro.at[d - 1], y=yy)

    basis_from_x(QB, snd.at[1], rxq, one.at[2])
    basis_whole(QB, one.at[2])
    put_qb = local(QB, qb_out, 7)
    send_z(WG, fs, snd.at[9], rzw)
    get_x.wait()
    left(vx, QB, lqt, 256 if QB.shape[3] % 256 == 0 else QB.shape[3])
    get_qc.wait()
    for yy in range(Y):
        both = dot(lqt[...], vqc[:, yy * 2 * q_cols : (yy + 1) * 2 * q_cols])
        low, high = both[:, :q_cols], both[:, q_cols:]
        psq[yy] = jnp.where(c == 0, high, low).astype(BF16)
        to(psq.at[yy], prq.at[yy], snd.at[4], s_prq.at[yy], c=other)
        mq[yy] = jnp.where(c == 0, low, high)
    for yy in range(Y):
        received(prq.at[yy], s_prq.at[yy])
        both = mq[yy] + prq[yy].astype(F32)
        by_row = both.reshape(Z, X, rank_rows, q_cols).astype(BF16)
        for xx in range(X):
            xsq[xx, :, yy] = by_row[:, xx]
    for d in xs:
        xx = up(x, d, X)
        to(xsq.at[xx], xrq.at[d - 1], snd.at[5], s_xrq.at[d - 1], x=xx)

    total = yso[0].astype(F32)
    for d in ys:
        received(yro.at[d - 1], s_yro.at[d - 1])
        total = total + yro[d - 1].astype(F32)
    by_row = total.astype(BF16).reshape(Z, X, rank_rows, o_cols)
    for xx in range(X):
        xso[xx] = by_row[:, xx]
    for d in xs:
        xx = up(x, d, X)
        to(xso.at[xx], xro.at[d - 1], snd.at[6], s_xro.at[d - 1], x=xx)

    send_x(WG, fs, snd.at[9], lambda e: one.at[3])
    for d in zs:
        block = down(z, d, Z) * X + x
        received(WG.at[block], rzw.at[d - 1])
        send_x(WG, block, snd.at[9], lambda e: one.at[3])

    total = xsq[x].astype(F32)
    for d in xs:
        received(xrq.at[d - 1], s_xrq.at[d - 1])
        total = total + xrq[d - 1].astype(F32)
    zsq[...] = total.astype(BF16)
    for d in zs:
        zz = up(z, d, Z)
        to(zsq.at[zz], zrq.at[d - 1], snd.at[7], s_zrq.at[d - 1], z=zz)

    total = xso[x].astype(F32)
    for d in xs:
        received(xro.at[d - 1], s_xro.at[d - 1])
        total = total + xro[d - 1].astype(F32)
    zso[...] = total.astype(BF16)
    for d in zs:
        zz = up(z, d, Z)
        to(zso.at[zz], zro.at[d - 1], snd.at[8], s_zro.at[d - 1], z=zz)

    total = zsq[z].astype(F32)
    for d in zs:
        received(zrq.at[d - 1], s_zrq.at[d - 1])
        total = total + zrq[d - 1].astype(F32)
    ysq[...] = total.astype(BF16)
    for d in ys:
        yy = up(y, d, Y)
        to(ysq.at[yy], yrq.at[d - 1], snd.at[11], s_yrq.at[d - 1], y=yy)

    def moments(reduced, mean, square, mean_out, square_out):
        mean_new = 0.8 * mean[...] + 0.2 * reduced
        square_new = 0.9 * square[...] + 0.1 * reduced * reduced
        mean_out[...] = mean_new
        square_out[...] = square_new
        return (mean_new / (jnp.sqrt(square_new) + 1e-08)).astype(BF16)

    total = zso[z].astype(F32)
    for d in zs:
        received(zro.at[d - 1], s_zro.at[d - 1])
        total = total + zro[d - 1].astype(F32)
    DG[fs, :, q_cols:] = moments(total * token_scale, om, os_, om_out, os_out)
    total = ysq[y].astype(F32)
    for d in ys:
        received(yrq.at[d - 1], s_yrq.at[d - 1])
        total = total + yrq[d - 1].astype(F32)
    DG[fs, :, :q_cols] = moments(total * token_scale, qm, qs, qm_out, qs_out)

    send_z(DG, fs, snd.at[10], rzg)
    send_x(DG, fs, snd.at[10], lambda e: one.at[4])
    for d in zs:
        block = down(z, d, Z) * X + x
        received(DG.at[block], rzg.at[d - 1])
        send_x(DG, block, snd.at[10], lambda e: one.at[4])

    received(WG.at[pl.ds(0, Z * (X - 1))], one.at[3])
    put_wg = local(WG, wg_out, 8)
    sent(OB.at[pl.ds(0, Z * X - 1)], snd.at[0])
    sent(QB.at[pl.ds(0, Z * X - 1)], snd.at[1])
    sent(pso, snd.at[2])
    sent(yro, snd.at[3])
    sent(psq, snd.at[4])
    sent(xrq, snd.at[5])
    sent(xro, snd.at[6])
    sent(zrq, snd.at[7])
    sent(zro, snd.at[8])
    sent(WG.at[pl.ds(0, Z * X - 1)], snd.at[9])
    sent(yrq, snd.at[11])
    received(DG.at[pl.ds(0, Z * (X - 1))], one.at[4])
    put_dg = local(DG, dg_out, 9)
    sent(DG.at[pl.ds(0, Z * X - 1)], snd.at[10])
    put_ob.wait()
    put_qb.wait()
    put_wg.wait()
    put_dg.wait()


def finish(X, qb_in, ob_in, wg_in, dg_in, qw, ow, qm, qs, om, os_, *refs):
    (q_step, qw_new, q_copy, o_step, ow_new, o_copy, qm_out, qs_out, om_out, os_out,
     QB, OB, WG, DG, qfull, ofull, vqc, voc, sem) = refs
    fs = lax.axis_index("z") * X + lax.axis_index("x")
    copies = []
    for number, (src, dst) in enumerate(((dg_in, DG), (qb_in, QB), (ob_in, OB), (wg_in, WG))):
        copies.append(pltpu.make_async_copy(src, dst, sem.at[number]))
        copies[-1].start()
    q_cols, o_cols = qm.shape[1], om.shape[1]
    q_rows, o_rows = qw.shape[0], ow.shape[0]
    blocks = QB.shape[0]
    for src, dst in ((qm, qm_out), (qs, qs_out), (om, om_out), (os_, os_out)):
        dst[...] = src[...]
    copies[0].wait()
    copies[1].wait()
    rank = QB.shape[3]
    full = dot(QB[...].reshape(-1, rank), DG[:, :, :q_cols].reshape(rank, q_cols))
    qfull[...] = full
    q_scale = lax.rsqrt(jnp.sum(full * full, axis=0, keepdims=True) / (blocks * q_rows) + 0.05)
    copies[2].wait()
    full = dot(OB[...].reshape(-1, rank), DG[:, :, q_cols:].reshape(rank, o_cols))
    ofull[...] = full
    o_scale = lax.rsqrt(jnp.sum(full * full, axis=0, keepdims=True) / (blocks * o_rows) + 0.05)
    copies[3].wait()
    vqc[...] = (
        WG[:, 0:q_rows, :].astype(F32) - 0.01 * (qfull[...] * q_scale).reshape(blocks, q_rows, q_cols)
    ).astype(BF16).reshape(blocks * q_rows, q_cols)
    put_q = pltpu.make_async_copy(vqc, q_copy, sem.at[4])
    put_q.start()
    for half in range(o_cols // q_cols):
        part = slice(half * q_cols, (half + 1) * q_cols)
        rows = slice(q_rows + half * o_rows, q_rows + (half + 1) * o_rows)
        voc[:, part] = (
            WG[:, rows, :].astype(F32) - 0.01 * (ofull[:, part] * o_scale[:, part]).reshape(blocks, o_rows, q_cols)
        ).astype(BF16).reshape(blocks * o_rows, q_cols)
    put_o = pltpu.make_async_copy(voc, o_copy, sem.at[5])
    put_o.start()
    step = qfull[pl.ds(pl.multiple_of(fs * q_rows, q_rows), q_rows), :] * q_scale
    q_step[...] = step
    qw_new[...] = qw[...] - 0.01 * step
    step = ofull[pl.ds(pl.multiple_of(fs * o_rows, o_rows), o_rows), :] * o_scale
    o_step[...] = step
    ow_new[...] = ow[...] - 0.01 * step
    put_q.wait()
    put_o.wait()


def shards(xin, qc, h, oc, qw, ow, qb, ob, qm, qs, om, os_):
    Z, X, Y, C = (lax.axis_size(name) for name in ("z", "x", "y", "c"))
    blocks = Z * X
    tokens, model = xin.shape
    rank = qb.shape[1]
    q_rows, o_rows, rank_rows = qw.shape[0], ow.shape[0], qm.shape[0]
    q_cols, o_cols = qw.shape[1], ow.shape[1]
    wide = h.shape[1]
    token_scale = (tokens * blocks * Y * C) ** (-0.5)
    halves = o_cols // q_cols
    w_rows = q_rows + halves * o_rows
    any_spec = pl.BlockSpec(memory_space=pl.ANY)
    vmem = pl.BlockSpec(memory_space=pltpu.VMEM)
    shape = jax.ShapeDtypeStruct
    qb_shape = (blocks, 2, q_rows // 2, rank)
    ob_shape = (blocks, 2, o_rows // 2, rank)
    wg_shape = (blocks, w_rows, q_cols)
    dg_shape = (blocks, rank_rows, q_cols + o_cols)
    buffer = lambda *dims: pltpu.VMEM(dims, BF16)
    dma = lambda *dims: pltpu.SemaphoreType.DMA(dims)
    outs = pl.pallas_call(
        functools.partial(exchange, (Z, X, Y, token_scale)),
        out_shape=[
            shape(qb_shape, BF16), shape(ob_shape, BF16), shape(wg_shape, BF16), shape(dg_shape, BF16),
            shape(qm.shape, F32), shape(qs.shape, F32), shape(om.shape, F32), shape(os_.shape, F32),
        ],
        in_specs=[any_spec] * 6 + [vmem] * 6,
        out_specs=[any_spec] * 4 + [vmem] * 4,
        scratch_shapes=[
            buffer(*qb_shape), buffer(*ob_shape), buffer(*wg_shape), buffer(*dg_shape),
            buffer(tokens, model), buffer(tokens, wide), buffer(tokens, wide), buffer(tokens, model),
            buffer(rank, tokens), buffer(rank, tokens),
            buffer(Y, rank, o_cols), buffer(Y, rank, o_cols),
            buffer(Y, rank, o_cols), buffer(Y - 1, rank, o_cols),
            buffer(X, Z, rank_rows, o_cols), buffer(X - 1, Z, rank_rows, o_cols),
            buffer(Z, rank_rows, o_cols), buffer(Z - 1, rank_rows, o_cols),
            buffer(Y, rank, q_cols), buffer(Y, rank, q_cols), pltpu.VMEM((Y, rank, q_cols), F32),
            buffer(X, Z, Y, rank_rows, q_cols), buffer(X - 1, Z, Y, rank_rows, q_cols),
            buffer(Z, Y, rank_rows, q_cols), buffer(Z - 1, Y, rank_rows, q_cols),
            buffer(Y, rank_rows, q_cols), buffer(Y - 1, rank_rows, q_cols),
            dma(10), dma(12), dma(Z - 1), dma(Z, X - 1), dma(Z - 1), dma(Z, X - 1), dma(Z - 1), dma(Z - 1), dma(5),
            dma(Y), dma(Y - 1), dma(X - 1), dma(Z - 1), dma(Y), dma(X - 1), dma(Z - 1), dma(Y - 1),
        ],
        compiler_params=pltpu.CompilerParams(collective_id=0, has_side_effects=True, vmem_limit_bytes=LIMIT),
        name="exchange",
    )(
        xin, qc, h, oc, qb.reshape(qb_shape[1:]), ob.reshape(ob_shape[1:]),
        qw, ow, qm, qs, om, os_,
    )
    qb_all, ob_all, wg_all, dg_all, qm_new, qs_new, om_new, os_new = outs
    (q_step, qw_new, q_copy, o_step, ow_new, o_copy, qm_new, qs_new, om_new, os_new) = pl.pallas_call(
        functools.partial(finish, X),
        out_shape=[
            shape(qw.shape, F32), shape(qw.shape, F32), shape((blocks * q_rows, q_cols), BF16),
            shape(ow.shape, F32), shape(ow.shape, F32), shape((blocks * o_rows, o_cols), BF16),
            shape(qm.shape, F32), shape(qs.shape, F32), shape(om.shape, F32), shape(os_.shape, F32),
        ],
        in_specs=[any_spec] * 4 + [vmem] * 6,
        out_specs=[vmem, vmem, any_spec, vmem, vmem, any_spec] + [vmem] * 4,
        scratch_shapes=[
            buffer(*qb_shape), buffer(*ob_shape), buffer(*wg_shape), buffer(*dg_shape),
            pltpu.VMEM((blocks * q_rows, q_cols), F32), pltpu.VMEM((blocks * o_rows, o_cols), F32),
            buffer(blocks * q_rows, q_cols), buffer(blocks * o_rows, o_cols),
            dma(6),
        ],
        compiler_params=pltpu.CompilerParams(vmem_limit_bytes=LIMIT),
        name="finish",
    )(qb_all, ob_all, wg_all, dg_all, qw, ow, qm_new, qs_new, om_new, os_new)
    return (qm_new, qs_new, q_step, qw_new, q_copy, om_new, os_new, o_step, ow_new, o_copy)


def solution(mesh, split=(8, 4, 4, 2)):
    cube = Mesh(mesh.devices.reshape(split), FS_TP)
    tokens = P(FS_TP, None)
    tile = P(FS, TP)
    return jax.shard_map(
        shards,
        mesh=cube,
        in_specs=(tokens,) * 4 + (tile, tile, P(FS, None), P(FS, None)) + (tile,) * 4,
        out_specs=(tile, tile, tile, tile, P(None, TP), tile, tile, tile, tile, P(None, TP)),
        check_vma=False,
    )
```

```python
import functools

import jax
import jax.numpy as jnp
from jax import lax
from jax.experimental import pallas as pl
from jax.experimental.pallas import tpu as pltpu
from jax.sharding import Mesh
from jax.sharding import PartitionSpec as P

FS = ("z", "x")
FS_TP = ("z", "x", "y", "c")
TP = ("y", "c")
MESH = pl.DeviceIdType.MESH
F32 = jnp.float32
BF16 = jnp.bfloat16
LIMIT = 60 * 1024 * 1024


def nearest_first(n):
    return sorted(range(1, n), key=lambda d: (min(d, n - d), d))


def dot(a, b):
    return jnp.dot(a, b, preferred_element_type=F32)


def exchange(sizes, *refs):
    Z, X, Y, token_scale = sizes
    (xin, qcin, hin, ocin, qbin, obin, qw_in, ow_in, qm_in, qs_in, om_in, os_in,
     qb_out, ob_out, wg_out, dg_out, qm_out, qs_out, om_out, os_out,
     QB, OB, WG, DG, vx, vqc, vh, voc, lot, lqt, qw, ow, qm, qs, om, os_,
     pso, pro, mo, yso, ror, yro, xso, xro, zso, zro,
     psq, prq, mq, xsp, xrp, ysp, yrp, ysr, yrr, xsr, xrr, zsq, zrq,
     loc, snd, a_send, b_send, rzo, rxo, pro_d, rzq, rxq, prq_d, rzb, rxb, ryb, rgb, pb, rxw, rrw, rlw, rzg, one,
     s_pro, s_yrr, s_yro, s_xro, s_zro, s_prq, s_xrp, s_yrp, s_yrr2, s_xrr, s_zrq) = refs
    z, x, y, c = (lax.axis_index(name) for name in ("z", "x", "y", "c"))
    other = 1 - c
    rank_rows, q_cols = qm.shape
    o_cols = om.shape[1]
    q_rows, o_rows = qw.shape[0], ow.shape[0]

    def local(src, dst, number):
        copy = pltpu.make_async_copy(src, dst, loc.at[number])
        copy.start()
        return copy

    def to(src, dst, send, recv, **where):
        copy = pltpu.make_async_remote_copy(
            src_ref=src, dst_ref=dst, send_sem=send, recv_sem=recv, device_id=where, device_id_type=MESH
        )
        copy.start()

    def received(ref, recv):
        pltpu.make_async_remote_copy(
            src_ref=ref, dst_ref=ref, send_sem=snd.at[0], recv_sem=recv, device_id={"c": other}, device_id_type=MESH
        ).wait_recv()

    def sent(ref, send):
        pltpu.make_async_remote_copy(
            src_ref=ref, dst_ref=ref, send_sem=send, recv_sem=one.at[0], device_id={"c": other}, device_id_type=MESH
        ).wait_send()

    def up(at, d, n):
        return lax.rem(at + d, n)

    def down(at, d, n):
        return lax.rem(at + (n - d), n)

    zs, xs, ys = nearest_first(Z), nearest_first(X), nearest_first(Y)
    groups = [[0]] + [zs[at : at + 2] for at in range(0, len(zs), 2)]

    barrier = pltpu.get_barrier_semaphore()
    for d in zs:
        pl.semaphore_signal(barrier, inc=1, device_id={"z": up(z, d, Z)}, device_id_type=MESH)
    for d in xs:
        pl.semaphore_signal(barrier, inc=1, device_id={"x": up(x, d, X)}, device_id_type=MESH)
    for d in ys:
        pl.semaphore_signal(barrier, inc=1, device_id={"y": up(y, d, Y)}, device_id_type=MESH)
    pl.semaphore_signal(barrier, inc=1, device_id={"c": other}, device_id_type=MESH)

    half_rank = OB.shape[4]
    own = [
        local(src.at[:, pl.ds(half * half_rank, half_rank)], ref.at[z, x, half], number * 2 + half)
        for number, (src, ref) in enumerate(((obin, OB), (qbin, QB)))
        for half in range(2)
    ]
    small = [
        local(src, dst, 8 + number)
        for number, (src, dst) in enumerate(
            ((qw_in, qw), (ow_in, ow), (qm_in, qm), (qs_in, qs), (om_in, om), (os_in, os_))
        )
    ]
    get_h = local(hin, vh, 4)
    get_oc = local(ocin, voc, 5)
    get_x = local(xin, vx, 6)
    get_qc = local(qcin, vqc, 7)
    for copy in small + own:
        copy.wait()
    WG[z, x, 0:q_rows, :] = qw[...].astype(BF16)
    for half in range(o_cols // q_cols):
        WG[z, x, q_rows + half * o_rows : q_rows + (half + 1) * o_rows, :] = ow[
            :, half * q_cols : (half + 1) * q_cols
        ].astype(BF16)
    pl.semaphore_wait(barrier, len(zs) + len(xs) + len(ys) + 1)

    def pieces(ref, d, e, rows):
        return ref.at[down(z, d, Z), down(x, e, X), c, rows]

    class Gather:
        def __init__(self, ref, rows, send, rz, rx, pair):
            self.ref, self.rows, self.send, self.rz, self.rx, self.pair = ref, pl.ds(0, rows), send, rz, rx, pair

        def along_z(self):
            view = self.ref.at[z, x, c, self.rows]
            for d in zs:
                to(view, view, self.send.at[0], self.rz.at[d - 1], z=up(z, d, Z))

        def over(self, view, d):
            to(view, view, self.send.at[3 if d else 2], self.pair.at[d], c=other)

        def along_x(self, d):
            view = pieces(self.ref, d, 0, self.rows)
            if d:
                received(view, self.rz.at[d - 1])
            for e in xs:
                to(view, view, self.send.at[1], self.rx.at[d, e - 1], x=up(x, e, X))
            if d:
                self.over(view, d)

        def arrive(self, d):
            for e in xs:
                view = pieces(self.ref, d, e, self.rows)
                received(view, self.rx.at[d, e - 1])
                self.over(view, d)

        def whole(self):
            for d in [0] + zs:
                block = self.ref.at[0, pl.ds(0, X if d else X - 1), 0, self.rows]
                received(block, self.pair.at[d])

        def done(self):
            sent(self.ref.at[pl.ds(0, Z - 1), 0, 0, self.rows], self.send.at[0])
            sent(self.ref.at[:, pl.ds(0, X - 1), 0, self.rows], self.send.at[1])
            sent(self.ref.at[0, pl.ds(0, X - 1), 0, self.rows], self.send.at[2])
            sent(self.ref.at[pl.ds(0, Z - 1), :, 0, self.rows], self.send.at[3])

    class Shared:
        def __init__(self, ref, first, send):
            self.ref, self.first, self.send = ref, first, send
            self.each = (ref.shape[3] - first) // Y

        def rows(self, yy):
            return pl.ds(pl.multiple_of(self.first + yy * self.each, 8), self.each)

        def group(self, e, yy):
            return self.ref.at[:, down(x, e, X), c, self.rows(yy)]

        def along_z(self):
            view = self.ref.at[z, x, c, self.rows(y)]
            for d in zs:
                to(view, view, self.send.at[0], rzb.at[d - 1], z=up(z, d, Z))

        def along_x(self, d):
            view = pieces(self.ref, d, 0, self.rows(y))
            if d:
                received(view, rzb.at[d - 1])
            for e in xs:
                to(view, view, self.send.at[1], rxb.at[d, e - 1], x=up(x, e, X))
            if d:
                for f in ys:
                    to(view, view, self.send.at[2], ryb.at[d - 1, f - 1], y=up(y, f, Y))
                to(view, view, self.send.at[4], pb.at[0], c=other)

        def along_y(self):
            for e in xs:
                for d in [0] + zs:
                    received(pieces(self.ref, d, e, self.rows(y)), rxb.at[d, e - 1])
                view = self.group(e, y)
                for f in ys:
                    to(view, view, self.send.at[3], rgb.at[e - 1, f - 1], y=up(y, f, Y))
                to(view, view, self.send.at[5], pb.at[1], c=other)

        def arrive(self):
            for d in zs:
                for f in ys:
                    view = pieces(self.ref, d, 0, self.rows(down(y, f, Y)))
                    received(view, ryb.at[d - 1, f - 1])
                    to(view, view, self.send.at[4], pb.at[0], c=other)
            for e in xs:
                for f in ys:
                    view = self.group(e, down(y, f, Y))
                    received(view, rgb.at[e - 1, f - 1])
                    to(view, view, self.send.at[5], pb.at[1], c=other)

        def region(self, grouped, times):
            rows = pl.ds(self.first, times * self.each)
            return self.ref.at[:, pl.ds(0, X - 1), 0, rows] if grouped else self.ref.at[pl.ds(0, Z - 1), 0, 0, rows]

        def whole(self):
            received(self.region(False, Y), pb.at[0])
            received(self.region(True, Y), pb.at[1])

        def done(self):
            for number, (grouped, times) in enumerate(
                ((False, 1), (True, 1), (False, Y - 1), (True, Y - 1), (False, Y), (True, Y))
            ):
                sent(self.region(grouped, times), self.send.at[number])

    class Weights:
        rights, lefts = Z // 2, Z - 1 - Z // 2

        def along_x(self):
            for e in xs:
                to(WG.at[z, x], WG.at[z, x], snd.at[0], rxw.at[e - 1], x=up(x, e, X))

        def step(self, number):
            if number == 1:
                for e in xs:
                    received(WG.at[z, down(x, e, X)], rxw.at[e - 1])
            for count, recv, near, towards in (
                (self.rights, rrw, down(z, number - 1, Z), 1),
                (self.lefts, rlw, up(z, number - 1, Z), Z - 1),
            ):
                if 1 < number <= count + 1:
                    received(WG.at[near], recv.at[number - 2])
                if number <= count:
                    to(WG.at[near], WG.at[near], snd.at[1], recv.at[number - 1], z=up(z, towards, Z))

        def done(self):
            sent(WG.at[0, pl.ds(0, X - 1)], snd.at[0])
            sent(WG.at[pl.ds(0, Z - 1)], snd.at[1])

    gather_o = Gather(OB, o_rows, a_send.at[0], rzo, rxo, pro_d)
    gather_q = Gather(QB, q_rows // 2, a_send.at[1], rzq, rxq, prq_d)
    shared_q = Shared(QB, q_rows // 2, b_send)
    weights = Weights()
    steps = list(range(1, weights.rights + 2))

    def weights_step():
        if steps:
            weights.step(steps.pop(0))

    gather_o.along_z()
    gather_o.along_x(0)
    for number, d in enumerate(zs):
        gather_o.along_x(d)
        if number == min(1, len(zs) - 1):
            shared_q.along_z()
            gather_q.along_z()
    shared_q.along_x(0)
    gather_q.along_x(0)
    for group in groups[1:-1]:
        for d in group:
            shared_q.along_x(d)
            gather_q.along_x(d)
    for group in groups:
        for d in group:
            gather_o.arrive(d)

    def left(tokens, B, into, half):
        rows = B[:, :, half].reshape(-1, half_rank)
        count = tokens.shape[0] // 2
        for part in range(2):
            at = slice(part * count, (part + 1) * count)
            into[half, :, at] = dot(tokens[at], rows).astype(BF16).T

    get_h.wait()
    left(vh, OB, lot, c)
    for d in groups[-1]:
        shared_q.along_x(d)
        gather_q.along_x(d)
    gather_o.whole()
    put_ob = local(OB, ob_out, 14)
    left(vh, OB, lot, other)
    get_oc.wait()
    q_arrivals = list(groups)

    class Ring:
        def __init__(self, axis, at, n, S, R, N, far_send, send, s_r, s_n):
            self.axis, self.at, self.n, self.S, self.R, self.N = axis, at, n, S, R, N
            self.far_send, self.send, self.s_r, self.s_n = far_send, send, s_r, s_n

        def go(self, src, dst, send, recv, d):
            to(src, dst, send, recv, **{self.axis: up(self.at, d, self.n)})

        def far(self, half):
            if self.n == 4:
                self.go(self.S.at[2, half], self.R.at[half], self.far_send, self.s_r.at[half], 3 if half else 1)

        def near(self, d, half):
            last = self.n - 1
            if self.n == 2 or (d, half) in ((1, 1), (last, 0)):
                side = 0 if d == 1 else 1
                self.go(self.S.at[d, half], self.N.at[side, half], self.send, self.s_n.at[side, half], d)

        def merge(self, half):
            if self.n == 4:
                d = 3 if half else 1
                received(self.R.at[half], self.s_r.at[half])
                self.S[d, half] = (self.S[d, half].astype(F32) + self.R[half].astype(F32)).astype(BF16)
                self.go(self.S.at[d, half], self.N.at[half, half], self.send, self.s_n.at[half, half], d)

        def total(self, half):
            result = self.S[0, half].astype(F32)
            for side in range(1 if self.n == 2 else 2):
                received(self.N.at[side, half], self.s_n.at[side, half])
                result = result + self.N[side, half].astype(F32)
            return result

        def done(self):
            if self.n == 4:
                sent(self.R, self.far_send)
                sent(self.N, self.send)
            else:
                sent(self.N.at[0], self.send)

    ring_o = Ring("y", y, Y, yso, ror, yro, snd.at[12], snd.at[3], s_yrr, s_yro)

    rank = 2 * half_rank

    def part_o(number, d):
        yy = up(y, d, Y)
        at = pl.multiple_of(yy * 2 * o_cols, 2 * o_cols)
        both = dot(lot[...].reshape(rank, -1), voc[:, pl.ds(at, 2 * o_cols)])
        low, high = both[:, :o_cols], both[:, o_cols:]
        pso[number] = jnp.where(c == 0, high, low).astype(BF16)
        to(pso.at[number], pro.at[number], snd.at[2], s_pro.at[number], c=other)
        mo[number % 2] = jnp.where(c == 0, low, high)

    def pair_o(number, d):
        received(pro.at[number], s_pro.at[number])
        both = (mo[number % 2] + pro[number].astype(F32)).astype(BF16)
        for half in range(2):
            yso[d, half] = both[half * rank // 2 : (half + 1) * rank // 2]
            if d == 2:
                ring_o.far(half)
            elif d:
                ring_o.near(d, half)

    order = [2, 1, 3, 0] if Y == 4 else [1, 0]
    for number, d in enumerate(order):
        part_o(number, d)
        if number:
            pair_o(number - 1, order[number - 1])
        if number == 0:
            shared_q.along_y()
            weights.along_x()
        elif q_arrivals:
            for e in q_arrivals.pop(0):
                gather_q.arrive(e)
    pair_o(len(order) - 1, order[-1])

    for group in q_arrivals:
        for e in group:
            gather_q.arrive(e)
    weights_step()
    shared_q.arrive()
    get_x.wait()
    left(vx, QB, lqt, c)
    gather_q.whole()
    shared_q.whole()
    put_qb = local(QB, qb_out, 15)
    left(vx, QB, lqt, other)
    get_qc.wait()
    each = Y // 2
    for half in range(2):
        first = half * each
        wide = dot(lqt[...].reshape(rank, -1), vqc[:, first * 2 * q_cols : (first + each) * 2 * q_cols])
        for yy in range(first, first + each):
            at = (yy - first) * 2 * q_cols
            low, high = wide[:, at : at + q_cols], wide[:, at + q_cols : at + 2 * q_cols]
            psq[yy] = jnp.where(c == 0, high, low).astype(BF16)
            to(psq.at[yy], prq.at[yy], snd.at[4], s_prq.at[yy], c=other)
            mq[yy] = jnp.where(c == 0, low, high)
    for half in range(2):
        ring_o.merge(half)
    weights_step()
    low_rows = rank_rows // 2
    for d in ys + [0]:
        yy = up(y, d, Y)
        received(prq.at[yy], s_prq.at[yy])
        both = (mq[yy] + prq[yy].astype(F32)).reshape(Z, X, rank_rows, q_cols)
        for xx in range(X):
            xsp[xx, yy] = both[:, xx, :low_rows].astype(BF16)
            ysr[yy, xx] = both[:, xx, low_rows:].astype(BF16)
        if d:
            to(ysr.at[yy], yrr.at[d - 1], snd.at[5], s_yrr2.at[d - 1], y=yy)
    for d in xs:
        xx = up(x, d, X)
        to(xsp.at[xx], xrp.at[d - 1], snd.at[13], s_xrp.at[d - 1], x=xx)

    per = rank_rows * X
    rows = Z * X // 2
    for half in range(2):
        total = ring_o.total(half).astype(BF16).reshape(rows, rank_rows, o_cols)
        for row in range(rows):
            at = half * rows + row
            xso[at % X, at // X] = total[row]
    for d in xs:
        xx = up(x, d, X)
        to(xso.at[xx], xro.at[d - 1], snd.at[6], s_xro.at[d - 1], x=xx)
    weights_step()

    def summed(own, others, sems):
        total = own.astype(F32)
        for number in range(others.shape[0]):
            received(others.at[number], sems.at[number])
            total = total + others[number].astype(F32)
        return total

    xsr[...] = summed(ysr[y], yrr, s_yrr2).astype(BF16)
    for d in xs:
        xx = up(x, d, X)
        to(xsr.at[xx], xrr.at[d - 1], snd.at[9], s_xrr.at[d - 1], x=xx)
    ysp[...] = summed(xsp[x], xrp, s_xrp).astype(BF16)
    for d in ys:
        yy = up(y, d, Y)
        to(ysp.at[yy], yrp.at[d - 1], snd.at[11], s_yrp.at[d - 1], y=yy)

    total = xso[x].astype(F32)
    for d in xs:
        received(xro.at[d - 1], s_xro.at[d - 1])
        total = total + xro[d - 1].astype(F32)
    zso[...] = total.astype(BF16)
    for d in zs:
        zz = up(z, d, Z)
        to(zso.at[zz], zro.at[d - 1], snd.at[8], s_zro.at[d - 1], z=zz)

    zsq[:, low_rows:] = summed(xsr[x], xrr, s_xrr).astype(BF16)
    zsq[:, :low_rows] = summed(ysp[y], yrp, s_yrp).astype(BF16)
    for d in zs:
        zz = up(z, d, Z)
        to(zsq.at[zz], zrq.at[d - 1], snd.at[7], s_zrq.at[d - 1], z=zz)
    weights_step()

    def moments(reduced, mean, square):
        mean_new = 0.8 * mean[...] + 0.2 * reduced
        square_new = 0.9 * square[...] + 0.1 * reduced * reduced
        mean[...] = mean_new
        square[...] = square_new
        return (mean_new / (jnp.sqrt(square_new) + 1e-08)).astype(BF16)

    total = zso[z].astype(F32)
    for d in zs:
        received(zro.at[d - 1], s_zro.at[d - 1])
        total = total + zro[d - 1].astype(F32)
    DG[z, x, :, q_cols:] = moments(total * token_scale, om, os_)
    total = zsq[z].astype(F32)
    for d in zs:
        received(zrq.at[d - 1], s_zrq.at[d - 1])
        total = total + zrq[d - 1].astype(F32)
    DG[z, x, :, :q_cols] = moments(total * token_scale, qm, qs)

    def direction_x(d):
        view = DG.at[down(z, d, Z), x]
        if d:
            received(view, rzg.at[d - 1])
        for e in xs:
            to(view, view, snd.at[14], one.at[4], x=up(x, e, X))

    for d in zs:
        to(DG.at[z, x], DG.at[z, x], snd.at[10], rzg.at[d - 1], z=up(z, d, Z))
    direction_x(0)
    puts = [
        local(src, dst, number)
        for number, (src, dst) in enumerate(((qm, qm_out), (qs, qs_out), (om, om_out), (os_, os_out)))
    ]
    while steps:
        weights_step()
    for d in zs:
        direction_x(d)

    put_wg = local(WG, wg_out, 4)
    gather_o.done()
    gather_q.done()
    shared_q.done()
    weights.done()
    sent(pso, snd.at[2])
    ring_o.done()
    sent(psq, snd.at[4])
    sent(yrr, snd.at[5])
    sent(xrp, snd.at[13])
    sent(xrr, snd.at[9])
    sent(xro, snd.at[6])
    sent(zrq, snd.at[7])
    sent(zro, snd.at[8])
    sent(yrp, snd.at[11])
    put_ob.wait()
    put_qb.wait()
    for copy in puts:
        copy.wait()
    received(DG.at[:, pl.ds(0, X - 1)], one.at[4])
    put_dg = local(DG, dg_out, 5)
    sent(DG.at[pl.ds(0, Z - 1), 0], snd.at[10])
    sent(DG.at[:, pl.ds(0, X - 1)], snd.at[14])
    put_wg.wait()
    put_dg.wait()


def finish(X, qb_in, ob_in, wg_in, dg_in, qw, ow, qm, qs, om, os_, *refs):
    (q_step, qw_new, q_copy, o_step, ow_new, o_copy, qm_out, qs_out, om_out, os_out,
     QB, OB, WG, DG, qfull, ofull, vqc, voc, sem) = refs
    fs = lax.axis_index("z") * X + lax.axis_index("x")
    copies = []
    for number, (src, dst) in enumerate(((dg_in, DG), (qb_in, QB), (ob_in, OB), (wg_in, WG))):
        copies.append(pltpu.make_async_copy(src, dst, sem.at[number]))
        copies[-1].start()
    q_cols, o_cols = qm.shape[1], om.shape[1]
    q_rows, o_rows = qw.shape[0], ow.shape[0]
    blocks = QB.shape[0] * QB.shape[1]
    for src, dst in ((qm, qm_out), (qs, qs_out), (om, om_out), (os_, os_out)):
        dst[...] = src[...]
    copies[0].wait()
    copies[1].wait()
    half_rank = QB.shape[4]

    def product(B, columns):
        directions = DG[:, :, :, columns].reshape(2 * half_rank, -1)
        return sum(
            dot(B[:, :, half].reshape(-1, half_rank), directions[half * half_rank : (half + 1) * half_rank])
            for half in range(2)
        )

    full = product(QB, slice(0, q_cols))
    qfull[...] = full
    q_scale = lax.rsqrt(jnp.sum(full * full, axis=0, keepdims=True) / (blocks * q_rows) + 0.05)
    copies[2].wait()
    full = product(OB, slice(q_cols, q_cols + o_cols))
    ofull[...] = full
    o_scale = lax.rsqrt(jnp.sum(full * full, axis=0, keepdims=True) / (blocks * o_rows) + 0.05)
    copies[3].wait()
    vqc[...] = (
        WG[:, :, 0:q_rows].reshape(blocks, q_rows, q_cols).astype(F32) - 0.01 * (qfull[...] * q_scale).reshape(blocks, q_rows, q_cols)
    ).astype(BF16).reshape(blocks * q_rows, q_cols)
    put_q = pltpu.make_async_copy(vqc, q_copy, sem.at[4])
    put_q.start()
    for half in range(o_cols // q_cols):
        part = slice(half * q_cols, (half + 1) * q_cols)
        rows = slice(q_rows + half * o_rows, q_rows + (half + 1) * o_rows)
        voc[:, part] = (
            WG[:, :, rows].reshape(blocks, o_rows, q_cols).astype(F32) - 0.01 * (ofull[:, part] * o_scale[:, part]).reshape(blocks, o_rows, q_cols)
        ).astype(BF16).reshape(blocks * o_rows, q_cols)
    put_o = pltpu.make_async_copy(voc, o_copy, sem.at[5])
    put_o.start()
    step = qfull[pl.ds(pl.multiple_of(fs * q_rows, q_rows), q_rows), :] * q_scale
    q_step[...] = step
    qw_new[...] = qw[...] - 0.01 * step
    step = ofull[pl.ds(pl.multiple_of(fs * o_rows, o_rows), o_rows), :] * o_scale
    o_step[...] = step
    ow_new[...] = ow[...] - 0.01 * step
    put_q.wait()
    put_o.wait()


def shards(xin, qc, h, oc, qw, ow, qb, ob, qm, qs, om, os_):
    Z, X, Y, C = (lax.axis_size(name) for name in ("z", "x", "y", "c"))
    blocks = Z * X
    tokens, model = xin.shape
    rank = qb.shape[1]
    q_rows, o_rows, rank_rows = qw.shape[0], ow.shape[0], qm.shape[0]
    q_cols, o_cols = qw.shape[1], ow.shape[1]
    wide = h.shape[1]
    token_scale = (tokens * blocks * Y * C) ** (-0.5)
    halves = o_cols // q_cols
    w_rows = q_rows + halves * o_rows
    any_spec = pl.BlockSpec(memory_space=pl.ANY)
    vmem = pl.BlockSpec(memory_space=pltpu.VMEM)
    shape = jax.ShapeDtypeStruct
    qb_shape = (Z, X, 2, q_rows, rank // 2)
    ob_shape = (Z, X, 2, o_rows, rank // 2)
    wg_shape = (Z, X, w_rows, q_cols)
    dg_shape = (Z, X, rank_rows, q_cols + o_cols)
    near_z = max(Z - 1, 1)
    part_x = (X, Z, rank_rows // 2, q_cols)
    part_y = (Y, Z, rank_rows // 2, q_cols)
    buffer = lambda *dims: pltpu.VMEM(dims, BF16)
    dma = lambda *dims: pltpu.SemaphoreType.DMA(dims)
    outs = pl.pallas_call(
        functools.partial(exchange, (Z, X, Y, token_scale)),
        out_shape=[
            shape(qb_shape, BF16), shape(ob_shape, BF16), shape(wg_shape, BF16), shape(dg_shape, BF16),
            shape(qm.shape, F32), shape(qs.shape, F32), shape(om.shape, F32), shape(os_.shape, F32),
        ],
        in_specs=[any_spec] * 12,
        out_specs=[any_spec] * 8,
        scratch_shapes=[
            buffer(*qb_shape), buffer(*ob_shape), buffer(*wg_shape), buffer(*dg_shape),
            buffer(tokens, model), buffer(tokens, wide), buffer(tokens, wide), buffer(tokens, model),
            buffer(2, rank // 2, tokens), buffer(2, rank // 2, tokens),
            pltpu.VMEM(qw.shape, F32), pltpu.VMEM(ow.shape, F32), pltpu.VMEM(qm.shape, F32),
            pltpu.VMEM(qs.shape, F32), pltpu.VMEM(om.shape, F32), pltpu.VMEM(os_.shape, F32),
            buffer(Y, rank, o_cols), buffer(Y, rank, o_cols), pltpu.VMEM((2, rank, o_cols), F32),
            buffer(Y, 2, rank // 2, o_cols), buffer(2, rank // 2, o_cols), buffer(2, 2, rank // 2, o_cols),
            buffer(X, Z, rank_rows, o_cols), buffer(X - 1, Z, rank_rows, o_cols),
            buffer(Z, rank_rows, o_cols), buffer(near_z, rank_rows, o_cols),
            buffer(Y, rank, q_cols), buffer(Y, rank, q_cols), pltpu.VMEM((Y, rank, q_cols), F32),
            buffer(X, *part_y), buffer(X - 1, *part_y), buffer(*part_y), buffer(Y - 1, *part_y[1:]),
            buffer(Y, *part_x), buffer(Y - 1, *part_x), buffer(*part_x), buffer(X - 1, *part_x[1:]),
            buffer(Z, rank_rows, q_cols), buffer(near_z, rank_rows, q_cols),
            dma(16), dma(15), dma(2, 4), dma(6),
            dma(Z - 1), dma(Z, X - 1), dma(Z), dma(Z - 1), dma(Z, X - 1), dma(Z),
            dma(Z - 1), dma(Z, X - 1), dma(Z - 1, Y - 1), dma(X - 1, Y - 1), dma(2),
            dma(X - 1), dma(Z), dma(Z), dma(Z - 1), dma(5),
            dma(Y), dma(2), dma(2, 2), dma(X - 1), dma(near_z), dma(Y), dma(X - 1), dma(Y - 1), dma(Y - 1), dma(X - 1), dma(near_z),
        ],
        compiler_params=pltpu.CompilerParams(collective_id=0, has_side_effects=True, vmem_limit_bytes=LIMIT),
        name="exchange",
    )(
        xin, qc, h, oc, qb, ob,
        qw, ow, qm, qs, om, os_,
    )
    qb_all, ob_all, wg_all, dg_all, qm_new, qs_new, om_new, os_new = outs
    (q_step, qw_new, q_copy, o_step, ow_new, o_copy, qm_new, qs_new, om_new, os_new) = pl.pallas_call(
        functools.partial(finish, X),
        out_shape=[
            shape(qw.shape, F32), shape(qw.shape, F32), shape((blocks * q_rows, q_cols), BF16),
            shape(ow.shape, F32), shape(ow.shape, F32), shape((blocks * o_rows, o_cols), BF16),
            shape(qm.shape, F32), shape(qs.shape, F32), shape(om.shape, F32), shape(os_.shape, F32),
        ],
        in_specs=[any_spec] * 4 + [vmem] * 6,
        out_specs=[vmem, vmem, any_spec, vmem, vmem, any_spec] + [vmem] * 4,
        scratch_shapes=[
            buffer(*qb_shape), buffer(*ob_shape), buffer(*wg_shape), buffer(*dg_shape),
            pltpu.VMEM((blocks * q_rows, q_cols), F32), pltpu.VMEM((blocks * o_rows, o_cols), F32),
            buffer(blocks * q_rows, q_cols), buffer(blocks * o_rows, o_cols),
            dma(6),
        ],
        compiler_params=pltpu.CompilerParams(vmem_limit_bytes=LIMIT),
        name="finish",
    )(qb_all, ob_all, wg_all, dg_all, qw, ow, qm_new, qs_new, om_new, os_new)
    return (qm_new, qs_new, q_step, qw_new, q_copy, om_new, os_new, o_step, ow_new, o_copy)


def solution(mesh, split=(8, 4, 4, 2)):
    cube = Mesh(mesh.devices.reshape(split), FS_TP)
    tokens = P(FS_TP, None)
    tile = P(FS, TP)
    return jax.shard_map(
        shards,
        mesh=cube,
        in_specs=(tokens,) * 4 + (tile, tile, P(FS, None), P(FS, None)) + (tile,) * 4,
        out_specs=(tile, tile, tile, tile, P(None, TP), tile, tile, tile, tile, P(None, TP)),
        check_vma=False,
    )
```

```python
import functools

import jax
import jax.numpy as jnp
from jax import lax
from jax.experimental import pallas as pl
from jax.experimental.pallas import tpu as pltpu
from jax.sharding import Mesh
from jax.sharding import PartitionSpec as P

FS = ("z", "x")
FS_TP = ("z", "x", "y", "c")
TP = ("y", "c")
MESH = pl.DeviceIdType.MESH
F32 = jnp.float32
BF16 = jnp.bfloat16
LIMIT = 60 * 1024 * 1024


def nearest_first(n):
    return sorted(range(1, n), key=lambda d: (min(d, n - d), d))


def dot(a, b):
    return jnp.dot(a, b, preferred_element_type=F32)


def exchange(sizes, *refs):
    Z, X, Y, token_scale = sizes
    (xin, qcin, hin, ocin, qbin, obin, qw_in, ow_in, qm_in, qs_in, om_in, os_in,
     qb_out, ob_out, wg_out, do_out, dq_out, qm_out, qs_out, om_out, os_out,
     QB, OB, WG, DO, DQ, vx, vqc, vh, voc, lot, lqt, qw, ow, qm, qs, om, os_,
     pso, pro, mo, yso, ror, yro, xso, xro, zso, zro,
     psq, prq, mq, xsp, xrp, ysp, yrp, ysr, yrr, xsr, xrr, zsq, zrq,
     loc, snd, a_send, rzo, rxo, pro_d, rzq, rxq, prq_d, rxw, rrw, rlw, rzg, rzh, d_send, one,
     s_pro, s_yrr, s_yro, s_xro, s_zro, s_prq, s_xrp, s_yrp, s_yrr2, s_xrr, s_zrq) = refs
    z, x, y, c = (lax.axis_index(name) for name in ("z", "x", "y", "c"))
    other = 1 - c
    rank_rows, q_cols = qm.shape
    o_cols = om.shape[1]
    q_rows, o_rows = qw.shape[0], ow.shape[0]

    def local(src, dst, number):
        copy = pltpu.make_async_copy(src, dst, loc.at[number])
        copy.start()
        return copy

    def to(src, dst, send, recv, **where):
        copy = pltpu.make_async_remote_copy(
            src_ref=src, dst_ref=dst, send_sem=send, recv_sem=recv, device_id=where, device_id_type=MESH
        )
        copy.start()

    def received(ref, recv):
        pltpu.make_async_remote_copy(
            src_ref=ref, dst_ref=ref, send_sem=snd.at[0], recv_sem=recv, device_id={"c": other}, device_id_type=MESH
        ).wait_recv()

    def sent(ref, send):
        pltpu.make_async_remote_copy(
            src_ref=ref, dst_ref=ref, send_sem=send, recv_sem=one.at[0], device_id={"c": other}, device_id_type=MESH
        ).wait_send()

    def up(at, d, n):
        return lax.rem(at + d, n)

    def down(at, d, n):
        return lax.rem(at + (n - d), n)

    zs, xs, ys = nearest_first(Z), nearest_first(X), nearest_first(Y)
    groups = [[0]] + [zs[at : at + 2] for at in range(0, len(zs), 2)]

    barrier = pltpu.get_barrier_semaphore()
    for d in zs:
        pl.semaphore_signal(barrier, inc=1, device_id={"z": up(z, d, Z)}, device_id_type=MESH)
    for d in xs:
        pl.semaphore_signal(barrier, inc=1, device_id={"x": up(x, d, X)}, device_id_type=MESH)
    for d in ys:
        pl.semaphore_signal(barrier, inc=1, device_id={"y": up(y, d, Y)}, device_id_type=MESH)
    pl.semaphore_signal(barrier, inc=1, device_id={"c": other}, device_id_type=MESH)

    half_rank = OB.shape[4]
    own = [
        local(src.at[:, pl.ds(half * half_rank, half_rank)], ref.at[z, x, half], number * 2 + half)
        for number, (src, ref) in enumerate(((obin, OB), (qbin, QB)))
        for half in range(2)
    ]
    small = [
        local(src, dst, 8 + number)
        for number, (src, dst) in enumerate(
            ((qw_in, qw), (ow_in, ow), (qm_in, qm), (qs_in, qs), (om_in, om), (os_in, os_))
        )
    ]
    get_h = local(hin, vh, 4)
    get_oc = local(ocin, voc, 5)
    get_x = local(xin, vx, 6)
    get_qc = local(qcin, vqc, 7)
    for copy in small + own:
        copy.wait()
    WG[z, x, 0:q_rows, :] = qw[...].astype(BF16)
    for half in range(o_cols // q_cols):
        WG[z, x, q_rows + half * o_rows : q_rows + (half + 1) * o_rows, :] = ow[
            :, half * q_cols : (half + 1) * q_cols
        ].astype(BF16)
    pl.semaphore_wait(barrier, len(zs) + len(xs) + len(ys) + 1)

    def pieces(ref, d, e, rows):
        return ref.at[down(z, d, Z), down(x, e, X), c, rows]

    class Gather:
        def __init__(self, ref, rows, send, rz, rx, pair):
            self.ref, self.rows, self.send, self.rz, self.rx, self.pair = ref, pl.ds(0, rows), send, rz, rx, pair

        def along_z(self):
            view = self.ref.at[z, x, c, self.rows]
            for d in zs:
                to(view, view, self.send.at[0], self.rz.at[d - 1], z=up(z, d, Z))

        def over(self, view, d):
            to(view, view, self.send.at[3 if d else 2], self.pair.at[d], c=other)

        def along_x(self, d):
            view = pieces(self.ref, d, 0, self.rows)
            if d:
                received(view, self.rz.at[d - 1])
            for e in xs:
                to(view, view, self.send.at[1], self.rx.at[d, e - 1], x=up(x, e, X))
            if d:
                self.over(view, d)

        def arrive(self, d):
            for e in xs:
                view = pieces(self.ref, d, e, self.rows)
                received(view, self.rx.at[d, e - 1])
                self.over(view, d)

        def whole(self):
            for d in [0] + zs:
                block = self.ref.at[0, pl.ds(0, X if d else X - 1), 0, self.rows]
                received(block, self.pair.at[d])

        def done(self):
            sent(self.ref.at[pl.ds(0, Z - 1), 0, 0, self.rows], self.send.at[0])
            sent(self.ref.at[:, pl.ds(0, X - 1), 0, self.rows], self.send.at[1])
            sent(self.ref.at[0, pl.ds(0, X - 1), 0, self.rows], self.send.at[2])
            sent(self.ref.at[pl.ds(0, Z - 1), :, 0, self.rows], self.send.at[3])

    class Weights:
        rights, lefts = Z // 2, Z - 1 - Z // 2

        def along_x(self):
            for e in xs:
                to(WG.at[z, x], WG.at[z, x], snd.at[0], rxw.at[e - 1], x=up(x, e, X))

        def step(self, number):
            if number == 1:
                for e in xs:
                    received(WG.at[z, down(x, e, X)], rxw.at[e - 1])
            for count, recv, near, towards in (
                (self.rights, rrw, down(z, number - 1, Z), 1),
                (self.lefts, rlw, up(z, number - 1, Z), Z - 1),
            ):
                if 1 < number <= count + 1:
                    received(WG.at[near], recv.at[number - 2])
                if number <= count:
                    to(WG.at[near], WG.at[near], snd.at[1], recv.at[number - 1], z=up(z, towards, Z))

        def done(self):
            sent(WG.at[0, pl.ds(0, X - 1)], snd.at[0])
            sent(WG.at[pl.ds(0, Z - 1)], snd.at[1])

    gather_o = Gather(OB, o_rows, a_send.at[0], rzo, rxo, pro_d)
    gather_q = Gather(QB, q_rows, a_send.at[1], rzq, rxq, prq_d)
    weights = Weights()
    steps = list(range(1, weights.rights + 2))

    def weights_step():
        if steps:
            weights.step(steps.pop(0))

    gather_o.along_z()
    gather_o.along_x(0)
    for number, d in enumerate(zs):
        gather_o.along_x(d)
        if number == min(1, len(zs) - 1):
            gather_q.along_z()
    gather_q.along_x(0)
    for group in groups[1:-2]:
        for d in group:
            gather_q.along_x(d)
    for group in groups:
        for d in group:
            gather_o.arrive(d)

    def left(tokens, B, into, half):
        rows = B[:, :, half].reshape(-1, half_rank)
        count = tokens.shape[0] // 2
        for part in range(2):
            at = slice(part * count, (part + 1) * count)
            into[half, :, at] = dot(tokens[at], rows).astype(BF16).T

    get_h.wait()
    left(vh, OB, lot, c)
    for group in groups[max(1, len(groups) - 2) :]:
        for d in group:
            gather_q.along_x(d)
    gather_o.whole()
    put_ob = local(OB, ob_out, 14)
    left(vh, OB, lot, other)
    get_oc.wait()
    q_arrivals = list(groups)

    class Ring:
        def __init__(self, axis, at, n, S, R, N, far_send, send, s_r, s_n):
            self.axis, self.at, self.n, self.S, self.R, self.N = axis, at, n, S, R, N
            self.far_send, self.send, self.s_r, self.s_n = far_send, send, s_r, s_n

        def go(self, src, dst, send, recv, d):
            to(src, dst, send, recv, **{self.axis: up(self.at, d, self.n)})

        def far(self, half):
            if self.n == 4:
                self.go(self.S.at[2, half], self.R.at[half], self.far_send, self.s_r.at[half], 3 if half else 1)

        def near(self, d, half):
            last = self.n - 1
            if self.n == 2 or (d, half) in ((1, 1), (last, 0)):
                side = 0 if d == 1 else 1
                self.go(self.S.at[d, half], self.N.at[side, half], self.send, self.s_n.at[side, half], d)

        def merge(self, half):
            if self.n == 4:
                d = 3 if half else 1
                received(self.R.at[half], self.s_r.at[half])
                self.S[d, half] = (self.S[d, half].astype(F32) + self.R[half].astype(F32)).astype(BF16)
                self.go(self.S.at[d, half], self.N.at[half, half], self.send, self.s_n.at[half, half], d)

        def total(self, half):
            result = self.S[0, half].astype(F32)
            for side in range(1 if self.n == 2 else 2):
                received(self.N.at[side, half], self.s_n.at[side, half])
                result = result + self.N[side, half].astype(F32)
            return result

        def done(self):
            if self.n == 4:
                sent(self.R, self.far_send)
                sent(self.N, self.send)
            else:
                sent(self.N.at[0], self.send)

    ring_o = Ring("y", y, Y, yso, ror, yro, snd.at[12], snd.at[3], s_yrr, s_yro)

    rank = 2 * half_rank

    def part_o(number, d):
        yy = up(y, d, Y)
        at = pl.multiple_of(yy * 2 * o_cols, 2 * o_cols)
        both = dot(lot[...].reshape(rank, -1), voc[:, pl.ds(at, 2 * o_cols)])
        low, high = both[:, :o_cols], both[:, o_cols:]
        pso[number] = jnp.where(c == 0, high, low).astype(BF16)
        to(pso.at[number], pro.at[number], snd.at[2], s_pro.at[number], c=other)
        mo[number % 2] = jnp.where(c == 0, low, high)

    def pair_o(number, d):
        received(pro.at[number], s_pro.at[number])
        both = (mo[number % 2] + pro[number].astype(F32)).astype(BF16)
        for half in range(2):
            yso[d, half] = both[half * rank // 2 : (half + 1) * rank // 2]
            if d == 2:
                ring_o.far(half)
            elif d:
                ring_o.near(d, half)

    order = [2, 1, 3, 0] if Y == 4 else [1, 0]
    for number, d in enumerate(order):
        part_o(number, d)
        if number:
            pair_o(number - 1, order[number - 1])
        if number == 1:
            weights.along_x()
        if number and q_arrivals:
            for e in q_arrivals.pop(0):
                gather_q.arrive(e)
    pair_o(len(order) - 1, order[-1])

    for group in q_arrivals:
        for e in group:
            gather_q.arrive(e)
    weights_step()
    for half in range(2):
        ring_o.merge(half)
    get_x.wait()
    left(vx, QB, lqt, c)
    gather_q.whole()
    put_qb = local(QB, qb_out, 15)
    left(vx, QB, lqt, other)
    get_qc.wait()
    each = Y // 2
    for half in range(2):
        first = half * each
        wide = dot(lqt[...].reshape(rank, -1), vqc[:, first * 2 * q_cols : (first + each) * 2 * q_cols])
        for yy in range(first, first + each):
            at = (yy - first) * 2 * q_cols
            low, high = wide[:, at : at + q_cols], wide[:, at + q_cols : at + 2 * q_cols]
            psq[yy] = jnp.where(c == 0, high, low).astype(BF16)
            to(psq.at[yy], prq.at[yy], snd.at[4], s_prq.at[yy], c=other)
            mq[yy] = jnp.where(c == 0, low, high)
    weights_step()
    low_rows = rank_rows // 2
    for d in ys + [0]:
        yy = up(y, d, Y)
        received(prq.at[yy], s_prq.at[yy])
        both = (mq[yy] + prq[yy].astype(F32)).reshape(Z, X, rank_rows, q_cols)
        for xx in range(X):
            xsp[xx, yy] = both[:, xx, :low_rows].astype(BF16)
            ysr[yy, xx] = both[:, xx, low_rows:].astype(BF16)
        if d:
            to(ysr.at[yy], yrr.at[d - 1], snd.at[5], s_yrr2.at[d - 1], y=yy)
    for d in xs:
        xx = up(x, d, X)
        to(xsp.at[xx], xrp.at[d - 1], snd.at[13], s_xrp.at[d - 1], x=xx)

    per = rank_rows * X
    rows = Z * X // 2
    for half in range(2):
        total = ring_o.total(half).astype(BF16).reshape(rows, rank_rows, o_cols)
        for row in range(rows):
            at = half * rows + row
            xso[at % X, at // X] = total[row]
    for d in xs:
        xx = up(x, d, X)
        to(xso.at[xx], xro.at[d - 1], snd.at[6], s_xro.at[d - 1], x=xx)
    weights_step()

    def summed(own, others, sems):
        total = own.astype(F32)
        for number in range(others.shape[0]):
            received(others.at[number], sems.at[number])
            total = total + others[number].astype(F32)
        return total

    xsr[...] = summed(ysr[y], yrr, s_yrr2).astype(BF16)
    for d in xs:
        xx = up(x, d, X)
        to(xsr.at[xx], xrr.at[d - 1], snd.at[9], s_xrr.at[d - 1], x=xx)
    ysp[...] = summed(xsp[x], xrp, s_xrp).astype(BF16)
    for d in ys:
        yy = up(y, d, Y)
        to(ysp.at[yy], yrp.at[d - 1], snd.at[11], s_yrp.at[d - 1], y=yy)

    total = xso[x].astype(F32)
    for d in xs:
        received(xro.at[d - 1], s_xro.at[d - 1])
        total = total + xro[d - 1].astype(F32)
    zso[...] = total.astype(BF16)
    for d in zs:
        zz = up(z, d, Z)
        to(zso.at[zz], zro.at[d - 1], snd.at[8], s_zro.at[d - 1], z=zz)

    zsq[:, low_rows:] = summed(xsr[x], xrr, s_xrr).astype(BF16)
    zsq[:, :low_rows] = summed(ysp[y], yrp, s_yrp).astype(BF16)
    for d in zs:
        zz = up(z, d, Z)
        to(zsq.at[zz], zrq.at[d - 1], snd.at[7], s_zrq.at[d - 1], z=zz)
    weights_step()

    def moments(reduced, mean, square):
        mean_new = 0.8 * mean[...] + 0.2 * reduced
        square_new = 0.9 * square[...] + 0.1 * reduced * reduced
        mean[...] = mean_new
        square[...] = square_new
        return (mean_new / (jnp.sqrt(square_new) + 1e-08)).astype(BF16)

    total = zso[z].astype(F32)
    for d in zs:
        received(zro.at[d - 1], s_zro.at[d - 1])
        total = total + zro[d - 1].astype(F32)
    DO[z, x] = moments(total * token_scale, om, os_)

    class Directions:
        def __init__(self, ref, send, rz, rx):
            self.ref, self.send, self.rz, self.rx = ref, send, rz, rx

        def along_z(self):
            view = self.ref.at[z, x]
            for d in zs:
                to(view, view, self.send.at[0], self.rz.at[d - 1], z=up(z, d, Z))
            self.along_x(0)

        def along_x(self, d):
            view = self.ref.at[down(z, d, Z), x]
            if d:
                received(view, self.rz.at[d - 1])
            for e in xs:
                to(view, view, self.send.at[1], self.rx, x=up(x, e, X))

        def whole(self):
            received(self.ref.at[:, pl.ds(0, X - 1)], self.rx)

        def done(self):
            sent(self.ref.at[pl.ds(0, Z - 1), 0], self.send.at[0])
            sent(self.ref.at[:, pl.ds(0, X - 1)], self.send.at[1])

    gather_do = Directions(DO, d_send.at[0], rzg, one.at[4])
    gather_dq = Directions(DQ, d_send.at[1], rzh, one.at[3])
    gather_do.along_z()

    total = zsq[z].astype(F32)
    for d in zs:
        received(zrq.at[d - 1], s_zrq.at[d - 1])
        total = total + zrq[d - 1].astype(F32)
    DQ[z, x] = moments(total * token_scale, qm, qs)

    gather_dq.along_z()
    puts = [
        local(src, dst, number)
        for number, (src, dst) in enumerate(((qm, qm_out), (qs, qs_out), (om, om_out), (os_, os_out)))
    ]
    while steps:
        weights_step()
    for d in zs:
        gather_do.along_x(d)
    for d in zs:
        gather_dq.along_x(d)

    put_wg = local(WG, wg_out, 4)
    gather_o.done()
    gather_q.done()
    weights.done()
    sent(pso, snd.at[2])
    ring_o.done()
    sent(psq, snd.at[4])
    sent(yrr, snd.at[5])
    sent(xrp, snd.at[13])
    sent(xrr, snd.at[9])
    sent(xro, snd.at[6])
    sent(zrq, snd.at[7])
    sent(zro, snd.at[8])
    sent(yrp, snd.at[11])
    put_ob.wait()
    put_qb.wait()
    for copy in puts:
        copy.wait()
    gather_do.whole()
    put_do = local(DO, do_out, 5)
    gather_dq.whole()
    put_dq = local(DQ, dq_out, 6)
    gather_do.done()
    gather_dq.done()
    put_wg.wait()
    put_do.wait()
    put_dq.wait()


def finish(X, qb_in, ob_in, wg_in, do_in, dq_in, qw_in, ow_in, qm_in, qs_in, om_in, os_in, *refs):
    (q_step, qw_new, q_copy, o_step, ow_new, o_copy, qm_out, qs_out, om_out, os_out,
     QB, OB, WG, DO, DQ, qw, ow, qm, qs, om, os_, qstep, ostep, qfull, ofull, vqc, voc, sem) = refs
    fs = lax.axis_index("z") * X + lax.axis_index("x")
    q_cols, o_cols = qm.shape[1], om.shape[1]
    q_rows, o_rows = qw.shape[0], ow.shape[0]
    blocks = QB.shape[0] * QB.shape[1]
    half_rank = QB.shape[4]
    puts = []

    def local(src, dst, number):
        copy = pltpu.make_async_copy(src, dst, sem.at[number])
        copy.start()
        return copy

    pairs = (
        (dq_in, DQ), (qb_in, QB), (do_in, DO), (ob_in, OB), (wg_in, WG), (qw_in, qw), (ow_in, ow),
        (qm_in, qm), (qs_in, qs), (om_in, om), (os_in, os_),
    )
    gets = [local(src, dst, number) for number, (src, dst) in enumerate(pairs)]

    def product(B, D):
        directions = D[...].reshape(2 * half_rank, -1)
        return sum(
            dot(B[:, :, half].reshape(-1, half_rank), directions[half * half_rank : (half + 1) * half_rank])
            for half in range(2)
        )

    for number in (0, 1):
        gets[number].wait()
    full = product(QB, DQ)
    qfull[...] = full
    scale = lax.rsqrt(jnp.sum(full * full, axis=0, keepdims=True) / (blocks * q_rows) + 0.05)
    for number in (4, 5):
        gets[number].wait()
    vqc[...] = (
        WG[:, :, 0:q_rows].reshape(blocks, q_rows, q_cols).astype(F32)
        - 0.01 * (qfull[...] * scale).reshape(blocks, q_rows, q_cols)
    ).astype(BF16).reshape(blocks * q_rows, q_cols)
    puts.append(local(vqc, q_copy, 11))
    step = qfull[pl.ds(pl.multiple_of(fs * q_rows, q_rows), q_rows), :] * scale
    qstep[...] = step
    qw[...] = qw[...] - 0.01 * step
    puts.append(local(qstep, q_step, 12))
    puts.append(local(qw, qw_new, 13))
    for number in (2, 3, 6, 7, 8, 9, 10):
        gets[number].wait()
    for number, (src, dst) in enumerate(((qm, qm_out), (qs, qs_out), (om, om_out), (os_, os_out))):
        puts.append(local(src, dst, 17 + number))
    full = product(OB, DO)
    ofull[...] = full
    scale = lax.rsqrt(jnp.sum(full * full, axis=0, keepdims=True) / (blocks * o_rows) + 0.05)
    for half in range(o_cols // q_cols):
        part = slice(half * q_cols, (half + 1) * q_cols)
        rows = slice(q_rows + half * o_rows, q_rows + (half + 1) * o_rows)
        voc[:, part] = (
            WG[:, :, rows].reshape(blocks, o_rows, q_cols).astype(F32)
            - 0.01 * (ofull[:, part] * scale[:, part]).reshape(blocks, o_rows, q_cols)
        ).astype(BF16).reshape(blocks * o_rows, q_cols)
    puts.append(local(voc, o_copy, 14))
    step = ofull[pl.ds(pl.multiple_of(fs * o_rows, o_rows), o_rows), :] * scale
    ostep[...] = step
    ow[...] = ow[...] - 0.01 * step
    puts.append(local(ostep, o_step, 15))
    puts.append(local(ow, ow_new, 16))
    for copy in puts:
        copy.wait()


def shards(xin, qc, h, oc, qw, ow, qb, ob, qm, qs, om, os_):
    Z, X, Y, C = (lax.axis_size(name) for name in ("z", "x", "y", "c"))
    blocks = Z * X
    tokens, model = xin.shape
    rank = qb.shape[1]
    q_rows, o_rows, rank_rows = qw.shape[0], ow.shape[0], qm.shape[0]
    q_cols, o_cols = qw.shape[1], ow.shape[1]
    wide = h.shape[1]
    token_scale = (tokens * blocks * Y * C) ** (-0.5)
    halves = o_cols // q_cols
    w_rows = q_rows + halves * o_rows
    any_spec = pl.BlockSpec(memory_space=pl.ANY)
    shape = jax.ShapeDtypeStruct
    qb_shape = (Z, X, 2, q_rows, rank // 2)
    ob_shape = (Z, X, 2, o_rows, rank // 2)
    wg_shape = (Z, X, w_rows, q_cols)
    do_shape = (Z, X, rank_rows, o_cols)
    dq_shape = (Z, X, rank_rows, q_cols)
    near_z = max(Z - 1, 1)
    part_x = (X, Z, rank_rows // 2, q_cols)
    part_y = (Y, Z, rank_rows // 2, q_cols)
    buffer = lambda *dims: pltpu.VMEM(dims, BF16)
    dma = lambda *dims: pltpu.SemaphoreType.DMA(dims)
    outs = pl.pallas_call(
        functools.partial(exchange, (Z, X, Y, token_scale)),
        out_shape=[
            shape(qb_shape, BF16), shape(ob_shape, BF16), shape(wg_shape, BF16), shape(do_shape, BF16),
            shape(dq_shape, BF16),
            shape(qm.shape, F32), shape(qs.shape, F32), shape(om.shape, F32), shape(os_.shape, F32),
        ],
        in_specs=[any_spec] * 12,
        out_specs=[any_spec] * 9,
        scratch_shapes=[
            buffer(*qb_shape), buffer(*ob_shape), buffer(*wg_shape), buffer(*do_shape), buffer(*dq_shape),
            buffer(tokens, model), buffer(tokens, wide), buffer(tokens, wide), buffer(tokens, model),
            buffer(2, rank // 2, tokens), buffer(2, rank // 2, tokens),
            pltpu.VMEM(qw.shape, F32), pltpu.VMEM(ow.shape, F32), pltpu.VMEM(qm.shape, F32),
            pltpu.VMEM(qs.shape, F32), pltpu.VMEM(om.shape, F32), pltpu.VMEM(os_.shape, F32),
            buffer(Y, rank, o_cols), buffer(Y, rank, o_cols), pltpu.VMEM((2, rank, o_cols), F32),
            buffer(Y, 2, rank // 2, o_cols), buffer(2, rank // 2, o_cols), buffer(2, 2, rank // 2, o_cols),
            buffer(X, Z, rank_rows, o_cols), buffer(X - 1, Z, rank_rows, o_cols),
            buffer(Z, rank_rows, o_cols), buffer(near_z, rank_rows, o_cols),
            buffer(Y, rank, q_cols), buffer(Y, rank, q_cols), pltpu.VMEM((Y, rank, q_cols), F32),
            buffer(X, *part_y), buffer(X - 1, *part_y), buffer(*part_y), buffer(Y - 1, *part_y[1:]),
            buffer(Y, *part_x), buffer(Y - 1, *part_x), buffer(*part_x), buffer(X - 1, *part_x[1:]),
            buffer(Z, rank_rows, q_cols), buffer(near_z, rank_rows, q_cols),
            dma(16), dma(15), dma(2, 4),
            dma(Z - 1), dma(Z, X - 1), dma(Z), dma(Z - 1), dma(Z, X - 1), dma(Z),
            dma(X - 1), dma(Z), dma(Z), dma(Z - 1), dma(Z - 1), dma(2, 2), dma(5),
            dma(Y), dma(2), dma(2, 2), dma(X - 1), dma(near_z), dma(Y), dma(X - 1), dma(Y - 1), dma(Y - 1), dma(X - 1), dma(near_z),
        ],
        compiler_params=pltpu.CompilerParams(collective_id=0, has_side_effects=True, vmem_limit_bytes=LIMIT),
        name="exchange",
    )(
        xin, qc, h, oc, qb, ob,
        qw, ow, qm, qs, om, os_,
    )
    qb_all, ob_all, wg_all, do_all, dq_all, qm_new, qs_new, om_new, os_new = outs
    (q_step, qw_new, q_copy, o_step, ow_new, o_copy, qm_new, qs_new, om_new, os_new) = pl.pallas_call(
        functools.partial(finish, X),
        out_shape=[
            shape(qw.shape, F32), shape(qw.shape, F32), shape((blocks * q_rows, q_cols), BF16),
            shape(ow.shape, F32), shape(ow.shape, F32), shape((blocks * o_rows, o_cols), BF16),
            shape(qm.shape, F32), shape(qs.shape, F32), shape(om.shape, F32), shape(os_.shape, F32),
        ],
        in_specs=[any_spec] * 11,
        out_specs=[any_spec] * 10,
        scratch_shapes=[
            buffer(*qb_shape), buffer(*ob_shape), buffer(*wg_shape), buffer(*do_shape), buffer(*dq_shape),
            pltpu.VMEM(qw.shape, F32), pltpu.VMEM(ow.shape, F32), pltpu.VMEM(qm.shape, F32),
            pltpu.VMEM(qs.shape, F32), pltpu.VMEM(om.shape, F32), pltpu.VMEM(os_.shape, F32),
            pltpu.VMEM(qw.shape, F32), pltpu.VMEM(ow.shape, F32),
            pltpu.VMEM((blocks * q_rows, q_cols), F32), pltpu.VMEM((blocks * o_rows, o_cols), F32),
            buffer(blocks * q_rows, q_cols), buffer(blocks * o_rows, o_cols),
            dma(21),
        ],
        compiler_params=pltpu.CompilerParams(vmem_limit_bytes=LIMIT),
        name="finish",
    )(qb_all, ob_all, wg_all, do_all, dq_all, qw, ow, qm_new, qs_new, om_new, os_new)
    return (qm_new, qs_new, q_step, qw_new, q_copy, om_new, os_new, o_step, ow_new, o_copy)


def solution(mesh, split=(8, 4, 4, 2)):
    cube = Mesh(mesh.devices.reshape(split), FS_TP)
    tokens = P(FS_TP, None)
    tile = P(FS, TP)
    return jax.shard_map(
        shards,
        mesh=cube,
        in_specs=(tokens,) * 4 + (tile, tile, P(FS, None), P(FS, None)) + (tile,) * 4,
        out_specs=(tile, tile, tile, tile, P(None, TP), tile, tile, tile, tile, P(None, TP)),
        check_vma=False,
    )
```

```python
import functools

import jax
import jax.numpy as jnp
from jax import lax
from jax.experimental import pallas as pl
from jax.experimental.pallas import tpu as pltpu
from jax.sharding import Mesh
from jax.sharding import PartitionSpec as P

FS = ("z", "x")
FS_TP = ("z", "x", "y", "c")
TP = ("y", "c")
MESH = pl.DeviceIdType.MESH
F32 = jnp.float32
BF16 = jnp.bfloat16
LIMIT = 62_300_000


def nearest_first(n):
    return sorted(range(1, n), key=lambda d: (min(d, n - d), d))


def dot(a, b):
    return jnp.dot(a, b, preferred_element_type=F32)


def exchange(sizes, *refs):
    Z, X, Y, token_scale = sizes
    (xin, qcin, hin, ocin, qbin, obin, qw_in, ow_in, qm_in, qs_in, om_in, os_in,
     QB, OB, WG, DO, DQ, qm, qs, om, os_,
     vx, vqc, vh, voc, lot, lqt, qw, ow,
     pso, pro, mo, yso, ror, yro, xso, xro, zso, zro,
     psq, prq, mq, xsp, xrp, ysp, yrp, ysr, yrr, xsr, xrr, zsq, zrq,
     loc, snd, a_send, rzo, rxo, pro_d, rzq, rxq, prq_d, rxw, rrw, rlw, rzg, rzh, d_send, one,
     s_pro, s_yrr, s_yro, s_xro, s_zro, s_prq, s_xrp, s_yrp, s_yrr2, s_xrr, s_zrq) = refs
    z, x, y, c = (lax.axis_index(name) for name in ("z", "x", "y", "c"))
    other = 1 - c
    rank_rows, q_cols = qm.shape
    o_cols = om.shape[1]
    q_rows, o_rows = qw.shape[0], ow.shape[0]

    def local(src, dst, number):
        copy = pltpu.make_async_copy(src, dst, loc.at[number])
        copy.start()
        return copy

    def to(src, dst, send, recv, **where):
        copy = pltpu.make_async_remote_copy(
            src_ref=src, dst_ref=dst, send_sem=send, recv_sem=recv, device_id=where, device_id_type=MESH
        )
        copy.start()

    def received(ref, recv):
        pltpu.make_async_remote_copy(
            src_ref=ref, dst_ref=ref, send_sem=snd.at[0], recv_sem=recv, device_id={"c": other}, device_id_type=MESH
        ).wait_recv()

    def sent(ref, send):
        pltpu.make_async_remote_copy(
            src_ref=ref, dst_ref=ref, send_sem=send, recv_sem=one.at[0], device_id={"c": other}, device_id_type=MESH
        ).wait_send()

    def up(at, d, n):
        return lax.rem(at + d, n)

    def down(at, d, n):
        return lax.rem(at + (n - d), n)

    zs, xs, ys = nearest_first(Z), nearest_first(X), nearest_first(Y)
    groups = [[0]] + [zs[at : at + 2] for at in range(0, len(zs), 2)]

    barrier = pltpu.get_barrier_semaphore()
    for d in zs:
        pl.semaphore_signal(barrier, inc=1, device_id={"z": up(z, d, Z)}, device_id_type=MESH)
    for d in xs:
        pl.semaphore_signal(barrier, inc=1, device_id={"x": up(x, d, X)}, device_id_type=MESH)
    for d in ys:
        pl.semaphore_signal(barrier, inc=1, device_id={"y": up(y, d, Y)}, device_id_type=MESH)
    pl.semaphore_signal(barrier, inc=1, device_id={"c": other}, device_id_type=MESH)

    half_rank = OB.shape[4]
    own = [
        local(src.at[:, pl.ds(half * half_rank, half_rank)], ref.at[z, x, half], number * 2 + half)
        for number, (src, ref) in enumerate(((obin, OB), (qbin, QB)))
        for half in range(2)
    ]
    small = [
        local(src, dst, 8 + number)
        for number, (src, dst) in enumerate(
            ((qw_in, qw), (ow_in, ow), (qm_in, qm), (qs_in, qs), (om_in, om), (os_in, os_))
        )
    ]
    get_h = local(hin, vh, 4)
    get_oc = local(ocin, voc, 5)
    get_x = local(xin, vx, 6)
    get_qc = local(qcin, vqc, 7)
    for copy in small + own:
        copy.wait()
    WG[z, x, 0:q_rows, :] = qw[...].astype(BF16)
    for half in range(o_cols // q_cols):
        WG[z, x, q_rows + half * o_rows : q_rows + (half + 1) * o_rows, :] = ow[
            :, half * q_cols : (half + 1) * q_cols
        ].astype(BF16)
    pl.semaphore_wait(barrier, len(zs) + len(xs) + len(ys) + 1)

    def pieces(ref, d, e, rows):
        return ref.at[down(z, d, Z), down(x, e, X), c, rows]

    class Gather:
        def __init__(self, ref, rows, send, rz, rx, pair):
            self.ref, self.rows, self.send, self.rz, self.rx, self.pair = ref, pl.ds(0, rows), send, rz, rx, pair

        def along_z(self):
            view = self.ref.at[z, x, c, self.rows]
            for d in zs:
                to(view, view, self.send.at[0], self.rz.at[d - 1], z=up(z, d, Z))

        def over(self, view, d):
            to(view, view, self.send.at[3 if d else 2], self.pair.at[d], c=other)

        def along_x(self, d):
            view = pieces(self.ref, d, 0, self.rows)
            if d:
                received(view, self.rz.at[d - 1])
            for e in xs:
                to(view, view, self.send.at[1], self.rx.at[d, e - 1], x=up(x, e, X))
            if d:
                self.over(view, d)

        def arrive(self, d):
            for e in xs:
                view = pieces(self.ref, d, e, self.rows)
                received(view, self.rx.at[d, e - 1])
                self.over(view, d)

        def whole(self):
            for d in [0] + zs:
                block = self.ref.at[0, pl.ds(0, X if d else X - 1), 0, self.rows]
                received(block, self.pair.at[d])

        def done(self):
            sent(self.ref.at[pl.ds(0, Z - 1), 0, 0, self.rows], self.send.at[0])
            sent(self.ref.at[:, pl.ds(0, X - 1), 0, self.rows], self.send.at[1])
            sent(self.ref.at[0, pl.ds(0, X - 1), 0, self.rows], self.send.at[2])
            sent(self.ref.at[pl.ds(0, Z - 1), :, 0, self.rows], self.send.at[3])

    class Weights:
        rights, lefts = Z // 2, Z - 1 - Z // 2

        def along_x(self):
            for e in xs:
                to(WG.at[z, x], WG.at[z, x], snd.at[0], rxw.at[e - 1], x=up(x, e, X))

        def step(self, number):
            if number == 1:
                for e in xs:
                    received(WG.at[z, down(x, e, X)], rxw.at[e - 1])
            for count, recv, near, towards in (
                (self.rights, rrw, down(z, number - 1, Z), 1),
                (self.lefts, rlw, up(z, number - 1, Z), Z - 1),
            ):
                if 1 < number <= count + 1:
                    received(WG.at[near], recv.at[number - 2])
                if number <= count:
                    to(WG.at[near], WG.at[near], snd.at[1], recv.at[number - 1], z=up(z, towards, Z))

        def done(self):
            sent(WG.at[0, pl.ds(0, X - 1)], snd.at[0])
            sent(WG.at[pl.ds(0, Z - 1)], snd.at[1])

    gather_o = Gather(OB, o_rows, a_send.at[0], rzo, rxo, pro_d)
    gather_q = Gather(QB, q_rows, a_send.at[1], rzq, rxq, prq_d)
    weights = Weights()
    steps = list(range(1, weights.rights + 2))

    def weights_step():
        if steps:
            weights.step(steps.pop(0))

    gather_o.along_z()
    gather_o.along_x(0)
    for number, d in enumerate(zs):
        gather_o.along_x(d)
        if number == min(1, len(zs) - 1):
            gather_q.along_z()
    gather_q.along_x(0)
    for group in groups[1:-2]:
        for d in group:
            gather_q.along_x(d)
    for group in groups:
        for d in group:
            gather_o.arrive(d)

    def left(tokens, B, into, half):
        rows = B[:, :, half].reshape(-1, half_rank)
        count = tokens.shape[0] // 2
        for part in range(2):
            at = slice(part * count, (part + 1) * count)
            into[half, :, at] = dot(tokens[at], rows).astype(BF16).T

    get_h.wait()
    left(vh, OB, lot, c)
    for group in groups[max(1, len(groups) - 2) :]:
        for d in group:
            gather_q.along_x(d)
    gather_o.whole()
    left(vh, OB, lot, other)
    get_oc.wait()
    q_arrivals = list(groups)

    class Ring:
        def __init__(self, axis, at, n, S, R, N, far_send, send, s_r, s_n):
            self.axis, self.at, self.n, self.S, self.R, self.N = axis, at, n, S, R, N
            self.far_send, self.send, self.s_r, self.s_n = far_send, send, s_r, s_n

        def go(self, src, dst, send, recv, d):
            to(src, dst, send, recv, **{self.axis: up(self.at, d, self.n)})

        def far(self, half):
            if self.n == 4:
                self.go(self.S.at[2, half], self.R.at[half], self.far_send, self.s_r.at[half], 3 if half else 1)

        def near(self, d, half):
            last = self.n - 1
            if self.n == 2 or (d, half) in ((1, 1), (last, 0)):
                side = 0 if d == 1 else 1
                self.go(self.S.at[d, half], self.N.at[side, half], self.send, self.s_n.at[side, half], d)

        def merge(self, half):
            if self.n == 4:
                d = 3 if half else 1
                received(self.R.at[half], self.s_r.at[half])
                self.S[d, half] = (self.S[d, half].astype(F32) + self.R[half].astype(F32)).astype(BF16)
                self.go(self.S.at[d, half], self.N.at[half, half], self.send, self.s_n.at[half, half], d)

        def total(self, half):
            result = self.S[0, half].astype(F32)
            for side in range(1 if self.n == 2 else 2):
                received(self.N.at[side, half], self.s_n.at[side, half])
                result = result + self.N[side, half].astype(F32)
            return result

        def done(self):
            if self.n == 4:
                sent(self.R, self.far_send)
                sent(self.N, self.send)
            else:
                sent(self.N.at[0], self.send)

    ring_o = Ring("y", y, Y, yso, ror, yro, snd.at[12], snd.at[3], s_yrr, s_yro)

    rank = 2 * half_rank

    def part_o(number, d):
        yy = up(y, d, Y)
        at = pl.multiple_of(yy * 2 * o_cols, 2 * o_cols)
        both = dot(lot[...].reshape(rank, -1), voc[:, pl.ds(at, 2 * o_cols)])
        low, high = both[:, :o_cols], both[:, o_cols:]
        pso[number] = jnp.where(c == 0, high, low).astype(BF16)
        to(pso.at[number], pro.at[number], snd.at[2], s_pro.at[number], c=other)
        mo[number % 2] = jnp.where(c == 0, low, high)

    def pair_o(number, d):
        received(pro.at[number], s_pro.at[number])
        both = (mo[number % 2] + pro[number].astype(F32)).astype(BF16)
        for half in range(2):
            yso[d, half] = both[half * rank // 2 : (half + 1) * rank // 2]
            if d == 2:
                ring_o.far(half)
            elif d:
                ring_o.near(d, half)

    order = [2, 1, 3, 0] if Y == 4 else [1, 0]
    for number, d in enumerate(order):
        part_o(number, d)
        if number:
            pair_o(number - 1, order[number - 1])
        if number == 1:
            weights.along_x()
        if number and q_arrivals:
            for e in q_arrivals.pop(0):
                gather_q.arrive(e)
    pair_o(len(order) - 1, order[-1])

    for group in q_arrivals:
        for e in group:
            gather_q.arrive(e)
    weights_step()
    for half in range(2):
        ring_o.merge(half)
    get_x.wait()
    left(vx, QB, lqt, c)
    gather_q.whole()
    left(vx, QB, lqt, other)
    get_qc.wait()
    each = Y // 2
    for half in range(2):
        first = half * each
        wide = dot(lqt[...].reshape(rank, -1), vqc[:, first * 2 * q_cols : (first + each) * 2 * q_cols])
        for yy in range(first, first + each):
            at = (yy - first) * 2 * q_cols
            low, high = wide[:, at : at + q_cols], wide[:, at + q_cols : at + 2 * q_cols]
            psq[yy] = jnp.where(c == 0, high, low).astype(BF16)
            to(psq.at[yy], prq.at[yy], snd.at[4], s_prq.at[yy], c=other)
            mq[yy] = jnp.where(c == 0, low, high)
    weights_step()
    low_rows = rank_rows // 2
    for d in ys + [0]:
        yy = up(y, d, Y)
        received(prq.at[yy], s_prq.at[yy])
        both = (mq[yy] + prq[yy].astype(F32)).reshape(Z, X, rank_rows, q_cols)
        for xx in range(X):
            xsp[xx, yy] = both[:, xx, :low_rows].astype(BF16)
            ysr[yy, xx] = both[:, xx, low_rows:].astype(BF16)
        if d:
            to(ysr.at[yy], yrr.at[d - 1], snd.at[5], s_yrr2.at[d - 1], y=yy)
    for d in xs:
        xx = up(x, d, X)
        to(xsp.at[xx], xrp.at[d - 1], snd.at[13], s_xrp.at[d - 1], x=xx)

    per = rank_rows * X
    rows = Z * X // 2
    for half in range(2):
        total = ring_o.total(half).astype(BF16).reshape(rows, rank_rows, o_cols)
        for row in range(rows):
            at = half * rows + row
            xso[at % X, at // X] = total[row]
    for d in xs:
        xx = up(x, d, X)
        to(xso.at[xx], xro.at[d - 1], snd.at[6], s_xro.at[d - 1], x=xx)
    weights_step()

    def summed(own, others, sems):
        total = own.astype(F32)
        for number in range(others.shape[0]):
            received(others.at[number], sems.at[number])
            total = total + others[number].astype(F32)
        return total

    xsr[...] = summed(ysr[y], yrr, s_yrr2).astype(BF16)
    for d in xs:
        xx = up(x, d, X)
        to(xsr.at[xx], xrr.at[d - 1], snd.at[9], s_xrr.at[d - 1], x=xx)
    ysp[...] = summed(xsp[x], xrp, s_xrp).astype(BF16)
    for d in ys:
        yy = up(y, d, Y)
        to(ysp.at[yy], yrp.at[d - 1], snd.at[11], s_yrp.at[d - 1], y=yy)

    total = xso[x].astype(F32)
    for d in xs:
        received(xro.at[d - 1], s_xro.at[d - 1])
        total = total + xro[d - 1].astype(F32)
    zso[...] = total.astype(BF16)
    for d in zs:
        zz = up(z, d, Z)
        to(zso.at[zz], zro.at[d - 1], snd.at[8], s_zro.at[d - 1], z=zz)

    zsq[:, low_rows:] = summed(xsr[x], xrr, s_xrr).astype(BF16)
    zsq[:, :low_rows] = summed(ysp[y], yrp, s_yrp).astype(BF16)
    for d in zs:
        zz = up(z, d, Z)
        to(zsq.at[zz], zrq.at[d - 1], snd.at[7], s_zrq.at[d - 1], z=zz)
    weights_step()

    def moments(reduced, mean, square):
        mean_new = 0.8 * mean[...] + 0.2 * reduced
        square_new = 0.9 * square[...] + 0.1 * reduced * reduced
        mean[...] = mean_new
        square[...] = square_new
        return (mean_new / (jnp.sqrt(square_new) + 1e-08)).astype(BF16)

    total = zso[z].astype(F32)
    for d in zs:
        received(zro.at[d - 1], s_zro.at[d - 1])
        total = total + zro[d - 1].astype(F32)
    DO[z, x] = moments(total * token_scale, om, os_)

    class Directions:
        def __init__(self, ref, send, rz, rx):
            self.ref, self.send, self.rz, self.rx = ref, send, rz, rx

        def along_z(self):
            view = self.ref.at[z, x]
            for d in zs:
                to(view, view, self.send.at[0], self.rz.at[d - 1], z=up(z, d, Z))
            self.along_x(0)

        def along_x(self, d):
            view = self.ref.at[down(z, d, Z), x]
            if d:
                received(view, self.rz.at[d - 1])
            for e in xs:
                to(view, view, self.send.at[1], self.rx, x=up(x, e, X))

        def whole(self):
            received(self.ref.at[:, pl.ds(0, X - 1)], self.rx)

        def done(self):
            sent(self.ref.at[pl.ds(0, Z - 1), 0], self.send.at[0])
            sent(self.ref.at[:, pl.ds(0, X - 1)], self.send.at[1])

    gather_do = Directions(DO, d_send.at[0], rzg, one.at[4])
    gather_dq = Directions(DQ, d_send.at[1], rzh, one.at[3])
    gather_do.along_z()

    total = zsq[z].astype(F32)
    for d in zs:
        received(zrq.at[d - 1], s_zrq.at[d - 1])
        total = total + zrq[d - 1].astype(F32)
    DQ[z, x] = moments(total * token_scale, qm, qs)

    gather_dq.along_z()
    while steps:
        weights_step()
    for d in zs:
        gather_do.along_x(d)
    for d in zs:
        gather_dq.along_x(d)

    gather_o.done()
    gather_q.done()
    weights.done()
    sent(pso, snd.at[2])
    ring_o.done()
    sent(psq, snd.at[4])
    sent(yrr, snd.at[5])
    sent(xrp, snd.at[13])
    sent(xrr, snd.at[9])
    sent(xro, snd.at[6])
    sent(zrq, snd.at[7])
    sent(zro, snd.at[8])
    sent(yrp, snd.at[11])
    gather_do.whole()
    gather_dq.whole()
    gather_do.done()
    gather_dq.done()


def finish(X, QB, OB, WG, DO, DQ, qw, ow, qm, qs, om, os_, *refs):
    (q_step, qw_new, q_copy, o_step, ow_new, o_copy, qm_out, qs_out, om_out, os_out,
     qstep, ostep, qnew, onew, qfull, ofull, vqc, voc, sem) = refs
    fs = lax.axis_index("z") * X + lax.axis_index("x")
    q_cols, o_cols = qm.shape[1], om.shape[1]
    q_rows, o_rows = qw.shape[0], ow.shape[0]
    blocks = QB.shape[0] * QB.shape[1]
    half_rank = QB.shape[4]
    puts = []

    def local(src, dst, number):
        copy = pltpu.make_async_copy(src, dst, sem.at[number])
        copy.start()
        return copy

    for number, (src, dst) in enumerate(((qm, qm_out), (qs, qs_out), (om, om_out), (os_, os_out))):
        puts.append(local(src, dst, 6 + number))

    def product(B, D):
        directions = D[...].reshape(2 * half_rank, -1)
        return sum(
            dot(B[:, :, half].reshape(-1, half_rank), directions[half * half_rank : (half + 1) * half_rank])
            for half in range(2)
        )

    full = product(QB, DQ)
    qfull[...] = full
    scale = lax.rsqrt(jnp.sum(full * full, axis=0, keepdims=True) / (blocks * q_rows) + 0.05)
    vqc[...] = (
        WG[:, :, 0:q_rows].reshape(blocks, q_rows, q_cols).astype(F32)
        - 0.01 * (qfull[...] * scale).reshape(blocks, q_rows, q_cols)
    ).astype(BF16).reshape(blocks * q_rows, q_cols)
    puts.append(local(vqc, q_copy, 0))
    step = qfull[pl.ds(pl.multiple_of(fs * q_rows, q_rows), q_rows), :] * scale
    qstep[...] = step
    qnew[...] = qw[...] - 0.01 * step
    puts.append(local(qstep, q_step, 1))
    puts.append(local(qnew, qw_new, 2))
    full = product(OB, DO)
    ofull[...] = full
    scale = lax.rsqrt(jnp.sum(full * full, axis=0, keepdims=True) / (blocks * o_rows) + 0.05)
    for half in range(o_cols // q_cols):
        part = slice(half * q_cols, (half + 1) * q_cols)
        rows = slice(q_rows + half * o_rows, q_rows + (half + 1) * o_rows)
        voc[:, part] = (
            WG[:, :, rows].reshape(blocks, o_rows, q_cols).astype(F32)
            - 0.01 * (ofull[:, part] * scale[:, part]).reshape(blocks, o_rows, q_cols)
        ).astype(BF16).reshape(blocks * o_rows, q_cols)
    puts.append(local(voc, o_copy, 3))
    step = ofull[pl.ds(pl.multiple_of(fs * o_rows, o_rows), o_rows), :] * scale
    ostep[...] = step
    onew[...] = ow[...] - 0.01 * step
    puts.append(local(ostep, o_step, 4))
    puts.append(local(onew, ow_new, 5))
    for copy in puts:
        copy.wait()


def shards(xin, qc, h, oc, qw, ow, qb, ob, qm, qs, om, os_):
    Z, X, Y, C = (lax.axis_size(name) for name in ("z", "x", "y", "c"))
    blocks = Z * X
    tokens, model = xin.shape
    rank = qb.shape[1]
    q_rows, o_rows, rank_rows = qw.shape[0], ow.shape[0], qm.shape[0]
    q_cols, o_cols = qw.shape[1], ow.shape[1]
    wide = h.shape[1]
    token_scale = (tokens * blocks * Y * C) ** (-0.5)
    halves = o_cols // q_cols
    w_rows = q_rows + halves * o_rows
    vmem = pl.BlockSpec(memory_space=pltpu.VMEM)
    any_spec = pl.BlockSpec(memory_space=pltpu.HBM)
    shape = jax.ShapeDtypeStruct
    qb_shape = (Z, X, 2, q_rows, rank // 2)
    ob_shape = (Z, X, 2, o_rows, rank // 2)
    wg_shape = (Z, X, w_rows, q_cols)
    do_shape = (Z, X, rank_rows, o_cols)
    dq_shape = (Z, X, rank_rows, q_cols)
    near_z = max(Z - 1, 1)
    part_x = (X, Z, rank_rows // 2, q_cols)
    part_y = (Y, Z, rank_rows // 2, q_cols)
    buffer = lambda *dims: pltpu.VMEM(dims, BF16)
    dma = lambda *dims: pltpu.SemaphoreType.DMA(dims)
    outs = pl.pallas_call(
        functools.partial(exchange, (Z, X, Y, token_scale)),
        out_shape=[
            pltpu.VMEM(qb_shape, BF16), pltpu.VMEM(ob_shape, BF16), pltpu.VMEM(wg_shape, BF16), pltpu.VMEM(do_shape, BF16),
            pltpu.VMEM(dq_shape, BF16),
            pltpu.VMEM(qm.shape, F32), pltpu.VMEM(qs.shape, F32), pltpu.VMEM(om.shape, F32), pltpu.VMEM(os_.shape, F32),
        ],
        in_specs=[any_spec] * 12,
        out_specs=[vmem] * 9,
        scratch_shapes=[
            buffer(tokens, model), buffer(tokens, wide), buffer(tokens, wide), buffer(tokens, model),
            buffer(2, rank // 2, tokens), buffer(2, rank // 2, tokens),
            pltpu.VMEM(qw.shape, F32), pltpu.VMEM(ow.shape, F32),
            buffer(Y, rank, o_cols), buffer(Y, rank, o_cols), pltpu.VMEM((2, rank, o_cols), F32),
            buffer(Y, 2, rank // 2, o_cols), buffer(2, rank // 2, o_cols), buffer(2, 2, rank // 2, o_cols),
            buffer(X, Z, rank_rows, o_cols), buffer(X - 1, Z, rank_rows, o_cols),
            buffer(Z, rank_rows, o_cols), buffer(near_z, rank_rows, o_cols),
            buffer(Y, rank, q_cols), buffer(Y, rank, q_cols), pltpu.VMEM((Y, rank, q_cols), F32),
            buffer(X, *part_y), buffer(X - 1, *part_y), buffer(*part_y), buffer(Y - 1, *part_y[1:]),
            buffer(Y, *part_x), buffer(Y - 1, *part_x), buffer(*part_x), buffer(X - 1, *part_x[1:]),
            buffer(Z, rank_rows, q_cols), buffer(near_z, rank_rows, q_cols),
            dma(16), dma(15), dma(2, 4),
            dma(Z - 1), dma(Z, X - 1), dma(Z), dma(Z - 1), dma(Z, X - 1), dma(Z),
            dma(X - 1), dma(Z), dma(Z), dma(Z - 1), dma(Z - 1), dma(2, 2), dma(5),
            dma(Y), dma(2), dma(2, 2), dma(X - 1), dma(near_z), dma(Y), dma(X - 1), dma(Y - 1), dma(Y - 1), dma(X - 1), dma(near_z),
        ],
        compiler_params=pltpu.CompilerParams(collective_id=0, has_side_effects=True, vmem_limit_bytes=LIMIT),
        name="exchange",
    )(
        xin, qc, h, oc, qb, ob,
        qw, ow, qm, qs, om, os_,
    )
    qb_all, ob_all, wg_all, do_all, dq_all, qm_new, qs_new, om_new, os_new = outs
    (q_step, qw_new, q_copy, o_step, ow_new, o_copy, qm_new, qs_new, om_new, os_new) = pl.pallas_call(
        functools.partial(finish, X),
        out_shape=[
            shape(qw.shape, F32), shape(qw.shape, F32), shape((blocks * q_rows, q_cols), BF16),
            shape(ow.shape, F32), shape(ow.shape, F32), shape((blocks * o_rows, o_cols), BF16),
            shape(qm.shape, F32), shape(qs.shape, F32), shape(om.shape, F32), shape(os_.shape, F32),
        ],
        in_specs=[vmem] * 11,
        out_specs=[any_spec] * 10,
        scratch_shapes=[
            pltpu.VMEM(qw.shape, F32), pltpu.VMEM(ow.shape, F32), pltpu.VMEM(qw.shape, F32), pltpu.VMEM(ow.shape, F32),
            pltpu.VMEM((blocks * q_rows, q_cols), F32), pltpu.VMEM((blocks * o_rows, o_cols), F32),
            buffer(blocks * q_rows, q_cols), buffer(blocks * o_rows, o_cols),
            dma(10),
        ],
        compiler_params=pltpu.CompilerParams(vmem_limit_bytes=LIMIT // 2),
        name="finish",
    )(qb_all, ob_all, wg_all, do_all, dq_all, qw, ow, qm_new, qs_new, om_new, os_new)
    return (qm_new, qs_new, q_step, qw_new, q_copy, om_new, os_new, o_step, ow_new, o_copy)


def solution(mesh, split=(8, 4, 4, 2)):
    cube = Mesh(mesh.devices.reshape(split), FS_TP)
    tokens = P(FS_TP, None)
    tile = P(FS, TP)
    return jax.shard_map(
        shards,
        mesh=cube,
        in_specs=(tokens,) * 4 + (tile, tile, P(FS, None), P(FS, None)) + (tile,) * 4,
        out_specs=(tile, tile, tile, tile, P(None, TP), tile, tile, tile, tile, P(None, TP)),
        check_vma=False,
    )
```

```python
import functools

import jax
import jax.numpy as jnp
from jax import lax
from jax.experimental import pallas as pl
from jax.experimental.pallas import tpu as pltpu
from jax.sharding import Mesh
from jax.sharding import PartitionSpec as P

FS = ("z", "x")
FS_TP = ("z", "x", "y", "c")
TP = ("y", "c")
MESH = pl.DeviceIdType.MESH
F32 = jnp.float32
BF16 = jnp.bfloat16
LIMIT = 62_300_000


def nearest_first(n):
    return sorted(range(1, n), key=lambda d: (min(d, n - d), d))


def dot(a, b):
    return jnp.dot(a, b, preferred_element_type=F32)


def exchange(sizes, *refs):
    Z, X, Y, token_scale = sizes
    (xin, qcin, hin, ocin, qbin, obin, qw_in, ow_in, qm_in, qs_in, om_in, os_in,
     QB, OB, WG, DO, DQ, qm, qs, om, os_,
     vx, vqc, vh, voc, lot, lqt, qw, ow,
     pso, pro, mo, yso, ror, yro, xso, xro, zso, zro,
     psq, prq, mq, xsp, xrp, ysp, yrp, ysr, yrr, xsr, xrr, zsq, zrq,
     loc, snd, a_send, rzo, rxo, pro_d, rzq, rxq, prq_d, rxw, rrw, rlw, rzg, rzh, d_send, one,
     s_pro, s_yrr, s_yro, s_xro, s_zro, s_prq, s_xrp, s_yrp, s_yrr2, s_xrr, s_zrq) = refs
    z, x, y, c = (lax.axis_index(name) for name in ("z", "x", "y", "c"))
    other = 1 - c
    rank_rows, q_cols = qm.shape
    o_cols = om.shape[1]
    q_rows, o_rows = qw.shape[0], ow.shape[0]

    def local(src, dst, number):
        copy = pltpu.make_async_copy(src, dst, loc.at[number])
        copy.start()
        return copy

    def to(src, dst, send, recv, **where):
        copy = pltpu.make_async_remote_copy(
            src_ref=src, dst_ref=dst, send_sem=send, recv_sem=recv, device_id=where, device_id_type=MESH
        )
        copy.start()

    def received(ref, recv):
        pltpu.make_async_remote_copy(
            src_ref=ref, dst_ref=ref, send_sem=snd.at[0], recv_sem=recv, device_id={"c": other}, device_id_type=MESH
        ).wait_recv()

    def sent(ref, send):
        pltpu.make_async_remote_copy(
            src_ref=ref, dst_ref=ref, send_sem=send, recv_sem=one.at[0], device_id={"c": other}, device_id_type=MESH
        ).wait_send()

    def up(at, d, n):
        return lax.rem(at + d, n)

    def down(at, d, n):
        return lax.rem(at + (n - d), n)

    zs, xs, ys = nearest_first(Z), nearest_first(X), nearest_first(Y)
    groups = [[0]] + [zs[at : at + 2] for at in range(0, len(zs), 2)]

    barrier = pltpu.get_barrier_semaphore()
    for d in zs:
        pl.semaphore_signal(barrier, inc=1, device_id={"z": up(z, d, Z)}, device_id_type=MESH)
    for d in xs:
        pl.semaphore_signal(barrier, inc=1, device_id={"x": up(x, d, X)}, device_id_type=MESH)
    for d in ys:
        pl.semaphore_signal(barrier, inc=1, device_id={"y": up(y, d, Y)}, device_id_type=MESH)
    pl.semaphore_signal(barrier, inc=1, device_id={"c": other}, device_id_type=MESH)

    half_rank = OB.shape[4]
    own = [
        local(src.at[:, pl.ds(half * half_rank, half_rank)], ref.at[z, x, half], number * 2 + half)
        for number, (src, ref) in enumerate(((obin, OB), (qbin, QB)))
        for half in range(2)
    ]
    small = [
        local(src, dst, 8 + number)
        for number, (src, dst) in enumerate(
            ((qw_in, qw), (ow_in, ow), (qm_in, qm), (qs_in, qs), (om_in, om), (os_in, os_))
        )
    ]
    get_h = local(hin, vh, 4)
    get_oc = local(ocin, voc, 5)
    get_x = local(xin, vx, 6)
    get_qc = local(qcin, vqc, 7)
    for copy in small + own:
        copy.wait()
    WG[z, x, 0:q_rows, :] = qw[...].astype(BF16)
    for half in range(o_cols // q_cols):
        WG[z, x, q_rows + half * o_rows : q_rows + (half + 1) * o_rows, :] = ow[
            :, half * q_cols : (half + 1) * q_cols
        ].astype(BF16)
    pl.semaphore_wait(barrier, len(zs) + len(xs) + len(ys) + 1)

    def pieces(ref, d, e, rows):
        return ref.at[down(z, d, Z), down(x, e, X), c, rows]

    class Gather:
        def __init__(self, ref, rows, send, rz, rx, pair):
            self.ref, self.rows, self.send, self.rz, self.rx, self.pair = ref, pl.ds(0, rows), send, rz, rx, pair

        def along_z(self):
            view = self.ref.at[z, x, c, self.rows]
            for d in zs:
                to(view, view, self.send.at[0], self.rz.at[d - 1], z=up(z, d, Z))

        def over(self, view, d):
            to(view, view, self.send.at[3 if d else 2], self.pair.at[d], c=other)

        def along_x(self, d):
            view = pieces(self.ref, d, 0, self.rows)
            if d:
                received(view, self.rz.at[d - 1])
            for e in xs:
                to(view, view, self.send.at[1], self.rx.at[d, e - 1], x=up(x, e, X))
            if d:
                self.over(view, d)

        def arrive(self, d):
            for e in xs:
                view = pieces(self.ref, d, e, self.rows)
                received(view, self.rx.at[d, e - 1])
                self.over(view, d)

        def whole(self):
            for d in [0] + zs:
                block = self.ref.at[0, pl.ds(0, X if d else X - 1), 0, self.rows]
                received(block, self.pair.at[d])

        def done(self):
            sent(self.ref.at[pl.ds(0, Z - 1), 0, 0, self.rows], self.send.at[0])
            sent(self.ref.at[:, pl.ds(0, X - 1), 0, self.rows], self.send.at[1])
            sent(self.ref.at[0, pl.ds(0, X - 1), 0, self.rows], self.send.at[2])
            sent(self.ref.at[pl.ds(0, Z - 1), :, 0, self.rows], self.send.at[3])

    class Weights:
        rights, lefts = Z // 2, Z - 1 - Z // 2

        def along_x(self):
            for e in xs:
                to(WG.at[z, x], WG.at[z, x], snd.at[0], rxw.at[e - 1], x=up(x, e, X))

        def step(self, number):
            if number == 1:
                for e in xs:
                    received(WG.at[z, down(x, e, X)], rxw.at[e - 1])
            for count, recv, near, towards in (
                (self.rights, rrw, down(z, number - 1, Z), 1),
                (self.lefts, rlw, up(z, number - 1, Z), Z - 1),
            ):
                if 1 < number <= count + 1:
                    received(WG.at[near], recv.at[number - 2])
                if number <= count:
                    to(WG.at[near], WG.at[near], snd.at[1], recv.at[number - 1], z=up(z, towards, Z))

        def done(self):
            sent(WG.at[0, pl.ds(0, X - 1)], snd.at[0])
            sent(WG.at[pl.ds(0, Z - 1)], snd.at[1])

    gather_o = Gather(OB, o_rows, a_send.at[0], rzo, rxo, pro_d)
    gather_q = Gather(QB, q_rows, a_send.at[1], rzq, rxq, prq_d)
    weights = Weights()
    steps = list(range(1, weights.rights + 2))

    def weights_step():
        if steps:
            weights.step(steps.pop(0))

    gather_o.along_z()
    gather_o.along_x(0)
    weights.along_x()
    for number, d in enumerate(zs):
        gather_o.along_x(d)
        if number == min(1, len(zs) - 1):
            gather_q.along_z()
    gather_q.along_x(0)
    for group in groups[1:-2]:
        for d in group:
            gather_q.along_x(d)
    for group in groups:
        for d in group:
            gather_o.arrive(d)

    def left(tokens, B, into, half):
        rows = B[:, :, half].reshape(-1, half_rank)
        count = tokens.shape[0] // 2
        for part in range(2):
            at = slice(part * count, (part + 1) * count)
            into[half, :, at] = dot(tokens[at], rows).astype(BF16).T

    get_h.wait()
    left(vh, OB, lot, c)
    for group in groups[max(1, len(groups) - 2) :]:
        for d in group:
            gather_q.along_x(d)
    gather_o.whole()
    left(vh, OB, lot, other)
    weights_step()
    get_oc.wait()
    q_arrivals = list(groups)

    class Ring:
        def __init__(self, axis, at, n, S, R, N, far_send, send, s_r, s_n):
            self.axis, self.at, self.n, self.S, self.R, self.N = axis, at, n, S, R, N
            self.far_send, self.send, self.s_r, self.s_n = far_send, send, s_r, s_n

        def go(self, src, dst, send, recv, d):
            to(src, dst, send, recv, **{self.axis: up(self.at, d, self.n)})

        def far(self, half):
            if self.n == 4:
                self.go(self.S.at[2, half], self.R.at[half], self.far_send, self.s_r.at[half], 3 if half else 1)

        def near(self, d, half):
            last = self.n - 1
            if self.n == 2 or (d, half) in ((1, 1), (last, 0)):
                side = 0 if d == 1 else 1
                self.go(self.S.at[d, half], self.N.at[side, half], self.send, self.s_n.at[side, half], d)

        def merge(self, half):
            if self.n == 4:
                d = 3 if half else 1
                received(self.R.at[half], self.s_r.at[half])
                self.S[d, half] = (self.S[d, half].astype(F32) + self.R[half].astype(F32)).astype(BF16)
                self.go(self.S.at[d, half], self.N.at[half, half], self.send, self.s_n.at[half, half], d)

        def total(self, half):
            result = self.S[0, half].astype(F32)
            for side in range(1 if self.n == 2 else 2):
                received(self.N.at[side, half], self.s_n.at[side, half])
                result = result + self.N[side, half].astype(F32)
            return result

        def done(self):
            if self.n == 4:
                sent(self.R, self.far_send)
                sent(self.N, self.send)
            else:
                sent(self.N.at[0], self.send)

    ring_o = Ring("y", y, Y, yso, ror, yro, snd.at[12], snd.at[3], s_yrr, s_yro)

    rank = 2 * half_rank

    def part_o(number, d):
        yy = up(y, d, Y)
        at = pl.multiple_of(yy * 2 * o_cols, 2 * o_cols)
        both = dot(lot[...].reshape(rank, -1), voc[:, pl.ds(at, 2 * o_cols)])
        low, high = both[:, :o_cols], both[:, o_cols:]
        pso[number] = jnp.where(c == 0, high, low).astype(BF16)
        to(pso.at[number], pro.at[number], snd.at[2], s_pro.at[number], c=other)
        mo[number % 2] = jnp.where(c == 0, low, high)

    def pair_o(number, d):
        received(pro.at[number], s_pro.at[number])
        both = (mo[number % 2] + pro[number].astype(F32)).astype(BF16)
        for half in range(2):
            yso[d, half] = both[half * rank // 2 : (half + 1) * rank // 2]
            if d == 2:
                ring_o.far(half)
            elif d:
                ring_o.near(d, half)

    order = [2, 1, 3, 0] if Y == 4 else [1, 0]
    for number, d in enumerate(order):
        part_o(number, d)
        if number:
            pair_o(number - 1, order[number - 1])
        if number and q_arrivals:
            for e in q_arrivals.pop(0):
                gather_q.arrive(e)
    pair_o(len(order) - 1, order[-1])

    for group in q_arrivals:
        for e in group:
            gather_q.arrive(e)
    weights_step()
    for half in range(2):
        ring_o.merge(half)
    get_x.wait()
    left(vx, QB, lqt, c)
    gather_q.whole()
    left(vx, QB, lqt, other)
    get_qc.wait()
    each = Y // 2
    for half in range(2):
        first = half * each
        wide = dot(lqt[...].reshape(rank, -1), vqc[:, first * 2 * q_cols : (first + each) * 2 * q_cols])
        for yy in range(first, first + each):
            at = (yy - first) * 2 * q_cols
            low, high = wide[:, at : at + q_cols], wide[:, at + q_cols : at + 2 * q_cols]
            psq[yy] = jnp.where(c == 0, high, low).astype(BF16)
            to(psq.at[yy], prq.at[yy], snd.at[4], s_prq.at[yy], c=other)
            mq[yy] = jnp.where(c == 0, low, high)
    weights_step()
    low_rows = rank_rows // 2
    for d in ys + [0]:
        yy = up(y, d, Y)
        received(prq.at[yy], s_prq.at[yy])
        both = (mq[yy] + prq[yy].astype(F32)).reshape(Z, X, rank_rows, q_cols)
        for xx in range(X):
            xsp[xx, yy] = both[:, xx, :low_rows].astype(BF16)
            ysr[yy, xx] = both[:, xx, low_rows:].astype(BF16)
        if d:
            to(ysr.at[yy], yrr.at[d - 1], snd.at[5], s_yrr2.at[d - 1], y=yy)
    for d in xs:
        xx = up(x, d, X)
        to(xsp.at[xx], xrp.at[d - 1], snd.at[13], s_xrp.at[d - 1], x=xx)

    per = rank_rows * X
    rows = Z * X // 2
    for half in range(2):
        total = ring_o.total(half).astype(BF16).reshape(rows, rank_rows, o_cols)
        for row in range(rows):
            at = half * rows + row
            xso[at % X, at // X] = total[row]
    for d in xs:
        xx = up(x, d, X)
        to(xso.at[xx], xro.at[d - 1], snd.at[6], s_xro.at[d - 1], x=xx)
    weights_step()

    def summed(own, others, sems):
        total = own.astype(F32)
        for number in range(others.shape[0]):
            received(others.at[number], sems.at[number])
            total = total + others[number].astype(F32)
        return total

    xsr[...] = summed(ysr[y], yrr, s_yrr2).astype(BF16)
    for d in xs:
        xx = up(x, d, X)
        to(xsr.at[xx], xrr.at[d - 1], snd.at[9], s_xrr.at[d - 1], x=xx)
    ysp[...] = summed(xsp[x], xrp, s_xrp).astype(BF16)
    for d in ys:
        yy = up(y, d, Y)
        to(ysp.at[yy], yrp.at[d - 1], snd.at[11], s_yrp.at[d - 1], y=yy)

    total = xso[x].astype(F32)
    for d in xs:
        received(xro.at[d - 1], s_xro.at[d - 1])
        total = total + xro[d - 1].astype(F32)
    zso[...] = total.astype(BF16)
    for d in zs:
        zz = up(z, d, Z)
        to(zso.at[zz], zro.at[d - 1], snd.at[8], s_zro.at[d - 1], z=zz)

    zsq[:, low_rows:] = summed(xsr[x], xrr, s_xrr).astype(BF16)
    zsq[:, :low_rows] = summed(ysp[y], yrp, s_yrp).astype(BF16)
    for d in zs:
        zz = up(z, d, Z)
        to(zsq.at[zz], zrq.at[d - 1], snd.at[7], s_zrq.at[d - 1], z=zz)

    def moments(reduced, mean, square):
        mean_new = 0.8 * mean[...] + 0.2 * reduced
        square_new = 0.9 * square[...] + 0.1 * reduced * reduced
        mean[...] = mean_new
        square[...] = square_new
        return (mean_new / (jnp.sqrt(square_new) + 1e-08)).astype(BF16)

    total = zso[z].astype(F32)
    for d in zs:
        received(zro.at[d - 1], s_zro.at[d - 1])
        total = total + zro[d - 1].astype(F32)
    DO[z, x] = moments(total * token_scale, om, os_)

    class Directions:
        def __init__(self, ref, send, rz, rx):
            self.ref, self.send, self.rz, self.rx = ref, send, rz, rx

        def along_z(self):
            view = self.ref.at[z, x]
            for d in zs:
                to(view, view, self.send.at[0], self.rz.at[d - 1], z=up(z, d, Z))
            self.along_x(0)

        def along_x(self, d):
            view = self.ref.at[down(z, d, Z), x]
            if d:
                received(view, self.rz.at[d - 1])
            for e in xs:
                to(view, view, self.send.at[1], self.rx, x=up(x, e, X))

        def whole(self):
            received(self.ref.at[:, pl.ds(0, X - 1)], self.rx)

        def done(self):
            sent(self.ref.at[pl.ds(0, Z - 1), 0], self.send.at[0])
            sent(self.ref.at[:, pl.ds(0, X - 1)], self.send.at[1])

    gather_do = Directions(DO, d_send.at[0], rzg, one.at[4])
    gather_dq = Directions(DQ, d_send.at[1], rzh, one.at[3])
    gather_do.along_z()

    total = zsq[z].astype(F32)
    for d in zs:
        received(zrq.at[d - 1], s_zrq.at[d - 1])
        total = total + zrq[d - 1].astype(F32)
    DQ[z, x] = moments(total * token_scale, qm, qs)

    gather_dq.along_z()
    while steps:
        weights_step()
    for d in zs:
        gather_do.along_x(d)
    for d in zs:
        gather_dq.along_x(d)

    gather_o.done()
    gather_q.done()
    weights.done()
    sent(pso, snd.at[2])
    ring_o.done()
    sent(psq, snd.at[4])
    sent(yrr, snd.at[5])
    sent(xrp, snd.at[13])
    sent(xrr, snd.at[9])
    sent(xro, snd.at[6])
    sent(zrq, snd.at[7])
    sent(zro, snd.at[8])
    sent(yrp, snd.at[11])
    gather_do.whole()
    gather_dq.whole()
    gather_do.done()
    gather_dq.done()


def finish(X, QB, OB, WG, DO, DQ, qw, ow, qm, qs, om, os_, *refs):
    (q_step, qw_new, q_copy, o_step, ow_new, o_copy, qm_out, qs_out, om_out, os_out,
     qstep, ostep, qnew, onew, qfull, ofull, vqc, voc, sem) = refs
    fs = lax.axis_index("z") * X + lax.axis_index("x")
    q_cols, o_cols = qm.shape[1], om.shape[1]
    q_rows, o_rows = qw.shape[0], ow.shape[0]
    blocks = QB.shape[0] * QB.shape[1]
    half_rank = QB.shape[4]
    puts = []

    def local(src, dst, number):
        copy = pltpu.make_async_copy(src, dst, sem.at[number])
        copy.start()
        return copy

    for number, (src, dst) in enumerate(((qm, qm_out), (qs, qs_out), (om, om_out), (os_, os_out))):
        puts.append(local(src, dst, 6 + number))

    def product(B, D):
        directions = D[...].reshape(2 * half_rank, -1)
        return sum(
            dot(B[:, :, half].reshape(-1, half_rank), directions[half * half_rank : (half + 1) * half_rank])
            for half in range(2)
        )

    full = product(QB, DQ)
    qfull[...] = full
    scale = lax.rsqrt(jnp.sum(full * full, axis=0, keepdims=True) / (blocks * q_rows) + 0.05)
    vqc[...] = (
        WG[:, :, 0:q_rows].reshape(blocks, q_rows, q_cols).astype(F32)
        - 0.01 * (qfull[...] * scale).reshape(blocks, q_rows, q_cols)
    ).astype(BF16).reshape(blocks * q_rows, q_cols)
    puts.append(local(vqc, q_copy, 0))
    step = qfull[pl.ds(pl.multiple_of(fs * q_rows, q_rows), q_rows), :] * scale
    qstep[...] = step
    qnew[...] = qw[...] - 0.01 * step
    puts.append(local(qstep, q_step, 1))
    puts.append(local(qnew, qw_new, 2))
    full = product(OB, DO)
    ofull[...] = full
    scale = lax.rsqrt(jnp.sum(full * full, axis=0, keepdims=True) / (blocks * o_rows) + 0.05)
    for half in range(o_cols // q_cols):
        part = slice(half * q_cols, (half + 1) * q_cols)
        rows = slice(q_rows + half * o_rows, q_rows + (half + 1) * o_rows)
        voc[:, part] = (
            WG[:, :, rows].reshape(blocks, o_rows, q_cols).astype(F32)
            - 0.01 * (ofull[:, part] * scale[:, part]).reshape(blocks, o_rows, q_cols)
        ).astype(BF16).reshape(blocks * o_rows, q_cols)
    puts.append(local(voc, o_copy, 3))
    step = ofull[pl.ds(pl.multiple_of(fs * o_rows, o_rows), o_rows), :] * scale
    ostep[...] = step
    onew[...] = ow[...] - 0.01 * step
    puts.append(local(ostep, o_step, 4))
    puts.append(local(onew, ow_new, 5))
    for copy in puts:
        copy.wait()


def shards(xin, qc, h, oc, qw, ow, qb, ob, qm, qs, om, os_):
    Z, X, Y, C = (lax.axis_size(name) for name in ("z", "x", "y", "c"))
    blocks = Z * X
    tokens, model = xin.shape
    rank = qb.shape[1]
    q_rows, o_rows, rank_rows = qw.shape[0], ow.shape[0], qm.shape[0]
    q_cols, o_cols = qw.shape[1], ow.shape[1]
    wide = h.shape[1]
    token_scale = (tokens * blocks * Y * C) ** (-0.5)
    halves = o_cols // q_cols
    w_rows = q_rows + halves * o_rows
    vmem = pl.BlockSpec(memory_space=pltpu.VMEM)
    any_spec = pl.BlockSpec(memory_space=pltpu.HBM)
    shape = jax.ShapeDtypeStruct
    qb_shape = (Z, X, 2, q_rows, rank // 2)
    ob_shape = (Z, X, 2, o_rows, rank // 2)
    wg_shape = (Z, X, w_rows, q_cols)
    do_shape = (Z, X, rank_rows, o_cols)
    dq_shape = (Z, X, rank_rows, q_cols)
    near_z = max(Z - 1, 1)
    part_x = (X, Z, rank_rows // 2, q_cols)
    part_y = (Y, Z, rank_rows // 2, q_cols)
    buffer = lambda *dims: pltpu.VMEM(dims, BF16)
    dma = lambda *dims: pltpu.SemaphoreType.DMA(dims)
    outs = pl.pallas_call(
        functools.partial(exchange, (Z, X, Y, token_scale)),
        out_shape=[
            pltpu.VMEM(qb_shape, BF16), pltpu.VMEM(ob_shape, BF16), pltpu.VMEM(wg_shape, BF16), pltpu.VMEM(do_shape, BF16),
            pltpu.VMEM(dq_shape, BF16),
            pltpu.VMEM(qm.shape, F32), pltpu.VMEM(qs.shape, F32), pltpu.VMEM(om.shape, F32), pltpu.VMEM(os_.shape, F32),
        ],
        in_specs=[any_spec] * 12,
        out_specs=[vmem] * 9,
        scratch_shapes=[
            buffer(tokens, model), buffer(tokens, wide), buffer(tokens, wide), buffer(tokens, model),
            buffer(2, rank // 2, tokens), buffer(2, rank // 2, tokens),
            pltpu.VMEM(qw.shape, F32), pltpu.VMEM(ow.shape, F32),
            buffer(Y, rank, o_cols), buffer(Y, rank, o_cols), pltpu.VMEM((2, rank, o_cols), F32),
            buffer(Y, 2, rank // 2, o_cols), buffer(2, rank // 2, o_cols), buffer(2, 2, rank // 2, o_cols),
            buffer(X, Z, rank_rows, o_cols), buffer(X - 1, Z, rank_rows, o_cols),
            buffer(Z, rank_rows, o_cols), buffer(near_z, rank_rows, o_cols),
            buffer(Y, rank, q_cols), buffer(Y, rank, q_cols), pltpu.VMEM((Y, rank, q_cols), F32),
            buffer(X, *part_y), buffer(X - 1, *part_y), buffer(*part_y), buffer(Y - 1, *part_y[1:]),
            buffer(Y, *part_x), buffer(Y - 1, *part_x), buffer(*part_x), buffer(X - 1, *part_x[1:]),
            buffer(Z, rank_rows, q_cols), buffer(near_z, rank_rows, q_cols),
            dma(16), dma(15), dma(2, 4),
            dma(Z - 1), dma(Z, X - 1), dma(Z), dma(Z - 1), dma(Z, X - 1), dma(Z),
            dma(X - 1), dma(Z), dma(Z), dma(Z - 1), dma(Z - 1), dma(2, 2), dma(5),
            dma(Y), dma(2), dma(2, 2), dma(X - 1), dma(near_z), dma(Y), dma(X - 1), dma(Y - 1), dma(Y - 1), dma(X - 1), dma(near_z),
        ],
        compiler_params=pltpu.CompilerParams(collective_id=0, has_side_effects=True, vmem_limit_bytes=LIMIT),
        name="exchange",
    )(
        xin, qc, h, oc, qb, ob,
        qw, ow, qm, qs, om, os_,
    )
    qb_all, ob_all, wg_all, do_all, dq_all, qm_new, qs_new, om_new, os_new = outs
    (q_step, qw_new, q_copy, o_step, ow_new, o_copy, qm_new, qs_new, om_new, os_new) = pl.pallas_call(
        functools.partial(finish, X),
        out_shape=[
            shape(qw.shape, F32), shape(qw.shape, F32), shape((blocks * q_rows, q_cols), BF16),
            shape(ow.shape, F32), shape(ow.shape, F32), shape((blocks * o_rows, o_cols), BF16),
            shape(qm.shape, F32), shape(qs.shape, F32), shape(om.shape, F32), shape(os_.shape, F32),
        ],
        in_specs=[vmem] * 11,
        out_specs=[any_spec] * 10,
        scratch_shapes=[
            pltpu.VMEM(qw.shape, F32), pltpu.VMEM(ow.shape, F32), pltpu.VMEM(qw.shape, F32), pltpu.VMEM(ow.shape, F32),
            pltpu.VMEM((blocks * q_rows, q_cols), F32), pltpu.VMEM((blocks * o_rows, o_cols), F32),
            buffer(blocks * q_rows, q_cols), buffer(blocks * o_rows, o_cols),
            dma(10),
        ],
        compiler_params=pltpu.CompilerParams(vmem_limit_bytes=LIMIT // 2),
        name="finish",
    )(qb_all, ob_all, wg_all, do_all, dq_all, qw, ow, qm_new, qs_new, om_new, os_new)
    return (qm_new, qs_new, q_step, qw_new, q_copy, om_new, os_new, o_step, ow_new, o_copy)


def solution(mesh, split=(8, 4, 4, 2)):
    cube = Mesh(mesh.devices.reshape(split), FS_TP)
    tokens = P(FS_TP, None)
    tile = P(FS, TP)
    return jax.shard_map(
        shards,
        mesh=cube,
        in_specs=(tokens,) * 4 + (tile, tile, P(FS, None), P(FS, None)) + (tile,) * 4,
        out_specs=(tile, tile, tile, tile, P(None, TP), tile, tile, tile, tile, P(None, TP)),
        check_vma=False,
    )
```

```python
import functools

import jax
import jax.numpy as jnp
from jax import lax
from jax.experimental import pallas as pl
from jax.experimental.pallas import tpu as pltpu
from jax.sharding import Mesh
from jax.sharding import PartitionSpec as P

FS = ("z", "x")
FS_TP = ("z", "x", "y", "c")
TP = ("y", "c")
MESH = pl.DeviceIdType.MESH
F32 = jnp.float32
BF16 = jnp.bfloat16
LIMIT = 62_300_000


def nearest_first(n):
    return sorted(range(1, n), key=lambda d: (min(d, n - d), d))


def dot(a, b):
    return jnp.dot(a, b, preferred_element_type=F32)


def exchange(sizes, *refs):
    Z, X, Y, token_scale = sizes
    (xin, qcin, hin, ocin, qbin, obin, qw_in, ow_in, qm_in, qs_in, om_in, os_in,
     QB, OB, WG, DO, DQ, qm, qs, om, os_,
     vx, vqc, vh, voc, lot, lqt, qw, ow, acc,
     pso, pro, mo, yso, ror, yro, xso, xro, zso, zro,
     psq, prq, mq, xsp, xrp, ysp, yrp, ysr, yrr, xsr, xrr, zsq, zrq,
     loc, snd, a_send, rzo, rxo, pro_d, rzq, rxq, prq_d, rxw, rrw, rlw, rzg, rzh, d_send, one,
     s_pro, s_yrr, s_yro, s_xro, s_zro, s_prq, s_xrp, s_yrp, s_yrr2, s_xrr, s_zrq) = refs
    z, x, y, c = (lax.axis_index(name) for name in ("z", "x", "y", "c"))
    other = 1 - c
    rank_rows, q_cols = qm.shape
    o_cols = om.shape[1]
    q_rows, o_rows = qw.shape[0], ow.shape[0]

    def local(src, dst, number):
        copy = pltpu.make_async_copy(src, dst, loc.at[number])
        copy.start()
        return copy

    def to(src, dst, send, recv, **where):
        copy = pltpu.make_async_remote_copy(
            src_ref=src, dst_ref=dst, send_sem=send, recv_sem=recv, device_id=where, device_id_type=MESH
        )
        copy.start()

    def received(ref, recv):
        pltpu.make_async_remote_copy(
            src_ref=ref, dst_ref=ref, send_sem=snd.at[0], recv_sem=recv, device_id={"c": other}, device_id_type=MESH
        ).wait_recv()

    def sent(ref, send):
        pltpu.make_async_remote_copy(
            src_ref=ref, dst_ref=ref, send_sem=send, recv_sem=one.at[0], device_id={"c": other}, device_id_type=MESH
        ).wait_send()

    def up(at, d, n):
        return lax.rem(at + d, n)

    def down(at, d, n):
        return lax.rem(at + (n - d), n)

    zs, xs, ys = nearest_first(Z), nearest_first(X), nearest_first(Y)
    groups = [[0]] + [zs[at : at + 2] for at in range(0, len(zs), 2)]

    barrier = pltpu.get_barrier_semaphore()
    for d in zs:
        pl.semaphore_signal(barrier, inc=1, device_id={"z": up(z, d, Z)}, device_id_type=MESH)
    for d in xs:
        pl.semaphore_signal(barrier, inc=1, device_id={"x": up(x, d, X)}, device_id_type=MESH)
    for d in ys:
        pl.semaphore_signal(barrier, inc=1, device_id={"y": up(y, d, Y)}, device_id_type=MESH)
    pl.semaphore_signal(barrier, inc=1, device_id={"c": other}, device_id_type=MESH)

    half_rank = OB.shape[4]
    own = [
        local(src.at[:, pl.ds(half * half_rank, half_rank)], ref.at[z, x, half], number * 2 + half)
        for number, (src, ref) in enumerate(((obin, OB), (qbin, QB)))
        for half in range(2)
    ]
    small = [
        local(src, dst, 8 + number)
        for number, (src, dst) in enumerate(
            ((qw_in, qw), (ow_in, ow), (qm_in, qm), (qs_in, qs), (om_in, om), (os_in, os_))
        )
    ]
    get_h = local(hin, vh, 4)
    get_oc = local(ocin, voc, 5)
    get_x = local(xin, vx, 6)
    get_qc = local(qcin, vqc, 7)
    for copy in small + own:
        copy.wait()
    WG[z, x, 0:q_rows, :] = qw[...].astype(BF16)
    for half in range(o_cols // q_cols):
        WG[z, x, q_rows + half * o_rows : q_rows + (half + 1) * o_rows, :] = ow[
            :, half * q_cols : (half + 1) * q_cols
        ].astype(BF16)
    pl.semaphore_wait(barrier, len(zs) + len(xs) + len(ys) + 1)

    def pieces(ref, d, e, rows):
        return ref.at[down(z, d, Z), down(x, e, X), c, rows]

    class Gather:
        def __init__(self, ref, rows, send, rz, rx, pair):
            self.ref, self.rows, self.send, self.rz, self.rx, self.pair = ref, pl.ds(0, rows), send, rz, rx, pair

        def along_z(self):
            view = self.ref.at[z, x, c, self.rows]
            for d in zs:
                to(view, view, self.send.at[0], self.rz.at[d - 1], z=up(z, d, Z))

        def over(self, view, d):
            to(view, view, self.send.at[3 if d else 2], self.pair.at[d], c=other)

        def along_x(self, d):
            view = pieces(self.ref, d, 0, self.rows)
            if d:
                received(view, self.rz.at[d - 1])
            for e in xs:
                to(view, view, self.send.at[1], self.rx.at[d, e - 1], x=up(x, e, X))
            if d:
                self.over(view, d)

        def arrive(self, d):
            for e in xs:
                view = pieces(self.ref, d, e, self.rows)
                received(view, self.rx.at[d, e - 1])
                self.over(view, d)

        def whole(self):
            for d in [0] + zs:
                block = self.ref.at[0, pl.ds(0, X if d else X - 1), 0, self.rows]
                received(block, self.pair.at[d])

        def done(self):
            sent(self.ref.at[pl.ds(0, Z - 1), 0, 0, self.rows], self.send.at[0])
            sent(self.ref.at[:, pl.ds(0, X - 1), 0, self.rows], self.send.at[1])
            sent(self.ref.at[0, pl.ds(0, X - 1), 0, self.rows], self.send.at[2])
            sent(self.ref.at[pl.ds(0, Z - 1), :, 0, self.rows], self.send.at[3])

    class Weights:
        rights, lefts = Z // 2, Z - 1 - Z // 2

        def along_x(self):
            for e in xs:
                to(WG.at[z, x], WG.at[z, x], snd.at[0], rxw.at[e - 1], x=up(x, e, X))

        def step(self, number):
            if number == 1:
                for e in xs:
                    received(WG.at[z, down(x, e, X)], rxw.at[e - 1])
            for count, recv, near, towards in (
                (self.rights, rrw, down(z, number - 1, Z), 1),
                (self.lefts, rlw, up(z, number - 1, Z), Z - 1),
            ):
                if 1 < number <= count + 1:
                    received(WG.at[near], recv.at[number - 2])
                if number <= count:
                    to(WG.at[near], WG.at[near], snd.at[1], recv.at[number - 1], z=up(z, towards, Z))

        def done(self):
            sent(WG.at[0, pl.ds(0, X - 1)], snd.at[0])
            sent(WG.at[pl.ds(0, Z - 1)], snd.at[1])

    gather_o = Gather(OB, o_rows, a_send.at[0], rzo, rxo, pro_d)
    gather_q = Gather(QB, q_rows, a_send.at[1], rzq, rxq, prq_d)
    weights = Weights()
    steps = list(range(1, weights.rights + 2))

    def weights_step():
        if steps:
            weights.step(steps.pop(0))

    gather_o.along_z()
    gather_o.along_x(0)
    weights.along_x()
    for number, d in enumerate(zs):
        gather_o.along_x(d)
        if number == min(1, len(zs) - 1):
            gather_q.along_z()
    gather_q.along_x(0)
    for group in groups[1:-2]:
        for d in group:
            gather_q.along_x(d)
    for group in groups:
        for d in group:
            gather_o.arrive(d)

    def left(tokens, B, into, half):
        rows = B[:, :, half].reshape(-1, half_rank)
        count = tokens.shape[0] // 2
        for part in range(2):
            at = slice(part * count, (part + 1) * count)
            into[half, :, at] = dot(tokens[at], rows).astype(BF16).T

    get_h.wait()
    left(vh, OB, lot, c)
    for group in groups[max(1, len(groups) - 2) :]:
        for d in group:
            gather_q.along_x(d)
    gather_o.whole()
    left(vh, OB, lot, other)
    weights_step()
    get_oc.wait()
    q_arrivals = list(groups)

    class Ring:
        def __init__(self, axis, at, n, S, R, N, far_send, send, s_r, s_n):
            self.axis, self.at, self.n, self.S, self.R, self.N = axis, at, n, S, R, N
            self.far_send, self.send, self.s_r, self.s_n = far_send, send, s_r, s_n

        def go(self, src, dst, send, recv, d):
            to(src, dst, send, recv, **{self.axis: up(self.at, d, self.n)})

        def far(self, half):
            if self.n == 4:
                self.go(self.S.at[2, half], self.R.at[half], self.far_send, self.s_r.at[half], 3 if half else 1)

        def near(self, d, half):
            last = self.n - 1
            if self.n == 2 or (d, half) in ((1, 1), (last, 0)):
                side = 0 if d == 1 else 1
                self.go(self.S.at[d, half], self.N.at[side, half], self.send, self.s_n.at[side, half], d)

        def merge(self, half):
            if self.n == 4:
                d = 3 if half else 1
                received(self.R.at[half], self.s_r.at[half])
                self.S[d, half] = (self.S[d, half].astype(F32) + self.R[half].astype(F32)).astype(BF16)
                self.go(self.S.at[d, half], self.N.at[half, half], self.send, self.s_n.at[half, half], d)

        def total(self, half):
            result = self.S[0, half].astype(F32)
            for side in range(1 if self.n == 2 else 2):
                received(self.N.at[side, half], self.s_n.at[side, half])
                result = result + self.N[side, half].astype(F32)
            return result

        def done(self):
            if self.n == 4:
                sent(self.R, self.far_send)
                sent(self.N, self.send)
            else:
                sent(self.N.at[0], self.send)

    ring_o = Ring("y", y, Y, yso, ror, yro, snd.at[12], snd.at[3], s_yrr, s_yro)

    rank = 2 * half_rank

    def part_o(number, d):
        yy = up(y, d, Y)
        at = pl.multiple_of(yy * 2 * o_cols, 2 * o_cols)
        both = dot(lot[...].reshape(rank, -1), voc[:, pl.ds(at, 2 * o_cols)])
        low, high = both[:, :o_cols], both[:, o_cols:]
        pso[number] = jnp.where(c == 0, high, low).astype(BF16)
        to(pso.at[number], pro.at[number], snd.at[2], s_pro.at[number], c=other)
        mo[number % 2] = jnp.where(c == 0, low, high)

    def pair_o(number, d):
        received(pro.at[number], s_pro.at[number])
        both = (mo[number % 2] + pro[number].astype(F32)).astype(BF16)
        for half in range(2):
            yso[d, half] = both[half * rank // 2 : (half + 1) * rank // 2]
            if d == 2:
                ring_o.far(half)
            elif d:
                ring_o.near(d, half)

    order = [2, 1, 3, 0] if Y == 4 else [1, 0]
    for number, d in enumerate(order):
        part_o(number, d)
        if number:
            pair_o(number - 1, order[number - 1])
        if number and q_arrivals:
            for e in q_arrivals.pop(0):
                gather_q.arrive(e)
    pair_o(len(order) - 1, order[-1])

    get_x.wait()
    place = X * q_rows

    def left_part(ds):
        for part in range(2):
            count = vx.shape[0] // 2
            at = slice(part * count, (part + 1) * count)
            total = None
            for d in ds:
                zz = down(z, d, Z)
                columns = pl.ds(pl.multiple_of(zz * place, place), place)
                term = dot(vx[at, columns], QB[zz, :, c].reshape(place, half_rank))
                total = term if total is None else total + term
            yield at, total

    here = [d for group in groups[: max(1, len(groups) - 2)] for d in group]
    rest = [d for group in groups[max(1, len(groups) - 2) :] for d in group]
    for at, total in left_part(here):
        acc[at] = total
    for group in q_arrivals:
        for e in group:
            gather_q.arrive(e)
    weights_step()
    for half in range(2):
        ring_o.merge(half)
    for at, total in left_part(rest):
        lqt[c, :, at] = (acc[at] + total).astype(BF16).T
    gather_q.whole()
    left(vx, QB, lqt, other)
    get_qc.wait()
    each = Y // 2
    for half in range(2):
        first = half * each
        wide = dot(lqt[...].reshape(rank, -1), vqc[:, first * 2 * q_cols : (first + each) * 2 * q_cols])
        for yy in range(first, first + each):
            at = (yy - first) * 2 * q_cols
            low, high = wide[:, at : at + q_cols], wide[:, at + q_cols : at + 2 * q_cols]
            psq[yy] = jnp.where(c == 0, high, low).astype(BF16)
            to(psq.at[yy], prq.at[yy], snd.at[4], s_prq.at[yy], c=other)
            mq[yy] = jnp.where(c == 0, low, high)
    weights_step()
    low_rows = rank_rows // 2
    for d in ys + [0]:
        yy = up(y, d, Y)
        received(prq.at[yy], s_prq.at[yy])
        both = (mq[yy] + prq[yy].astype(F32)).reshape(Z, X, rank_rows, q_cols)
        for xx in range(X):
            xsp[xx, yy] = both[:, xx, :low_rows].astype(BF16)
            ysr[yy, xx] = both[:, xx, low_rows:].astype(BF16)
        if d:
            to(ysr.at[yy], yrr.at[d - 1], snd.at[5], s_yrr2.at[d - 1], y=yy)
    for d in xs:
        xx = up(x, d, X)
        to(xsp.at[xx], xrp.at[d - 1], snd.at[13], s_xrp.at[d - 1], x=xx)

    per = rank_rows * X
    rows = Z * X // 2
    for half in range(2):
        total = ring_o.total(half).astype(BF16).reshape(rows, rank_rows, o_cols)
        for row in range(rows):
            at = half * rows + row
            xso[at % X, at // X] = total[row]
    for d in xs:
        xx = up(x, d, X)
        to(xso.at[xx], xro.at[d - 1], snd.at[6], s_xro.at[d - 1], x=xx)
    weights_step()

    def summed(own, others, sems):
        total = own.astype(F32)
        for number in range(others.shape[0]):
            received(others.at[number], sems.at[number])
            total = total + others[number].astype(F32)
        return total

    xsr[...] = summed(ysr[y], yrr, s_yrr2).astype(BF16)
    for d in xs:
        xx = up(x, d, X)
        to(xsr.at[xx], xrr.at[d - 1], snd.at[9], s_xrr.at[d - 1], x=xx)
    ysp[...] = summed(xsp[x], xrp, s_xrp).astype(BF16)
    for d in ys:
        yy = up(y, d, Y)
        to(ysp.at[yy], yrp.at[d - 1], snd.at[11], s_yrp.at[d - 1], y=yy)

    total = xso[x].astype(F32)
    for d in xs:
        received(xro.at[d - 1], s_xro.at[d - 1])
        total = total + xro[d - 1].astype(F32)
    zso[...] = total.astype(BF16)
    for d in zs:
        zz = up(z, d, Z)
        to(zso.at[zz], zro.at[d - 1], snd.at[8], s_zro.at[d - 1], z=zz)

    zsq[:, low_rows:] = summed(xsr[x], xrr, s_xrr).astype(BF16)
    zsq[:, :low_rows] = summed(ysp[y], yrp, s_yrp).astype(BF16)
    for d in zs:
        zz = up(z, d, Z)
        to(zsq.at[zz], zrq.at[d - 1], snd.at[7], s_zrq.at[d - 1], z=zz)

    def moments(reduced, mean, square):
        mean_new = 0.8 * mean[...] + 0.2 * reduced
        square_new = 0.9 * square[...] + 0.1 * reduced * reduced
        mean[...] = mean_new
        square[...] = square_new
        return (mean_new / (jnp.sqrt(square_new) + 1e-08)).astype(BF16)

    total = zso[z].astype(F32)
    for d in zs:
        received(zro.at[d - 1], s_zro.at[d - 1])
        total = total + zro[d - 1].astype(F32)
    DO[z, x] = moments(total * token_scale, om, os_)

    class Directions:
        def __init__(self, ref, send, rz, rx):
            self.ref, self.send, self.rz, self.rx = ref, send, rz, rx

        def along_z(self):
            view = self.ref.at[z, x]
            for d in zs:
                to(view, view, self.send.at[0], self.rz.at[d - 1], z=up(z, d, Z))
            self.along_x(0)

        def along_x(self, d):
            view = self.ref.at[down(z, d, Z), x]
            if d:
                received(view, self.rz.at[d - 1])
            for e in xs:
                to(view, view, self.send.at[1], self.rx, x=up(x, e, X))

        def whole(self):
            received(self.ref.at[:, pl.ds(0, X - 1)], self.rx)

        def done(self):
            sent(self.ref.at[pl.ds(0, Z - 1), 0], self.send.at[0])
            sent(self.ref.at[:, pl.ds(0, X - 1)], self.send.at[1])

    gather_do = Directions(DO, d_send.at[0], rzg, one.at[4])
    gather_dq = Directions(DQ, d_send.at[1], rzh, one.at[3])
    gather_do.along_z()

    total = zsq[z].astype(F32)
    for d in zs:
        received(zrq.at[d - 1], s_zrq.at[d - 1])
        total = total + zrq[d - 1].astype(F32)
    DQ[z, x] = moments(total * token_scale, qm, qs)

    gather_dq.along_z()
    while steps:
        weights_step()
    for d in zs:
        gather_do.along_x(d)
    for d in zs:
        gather_dq.along_x(d)

    gather_o.done()
    gather_q.done()
    weights.done()
    sent(pso, snd.at[2])
    ring_o.done()
    sent(psq, snd.at[4])
    sent(yrr, snd.at[5])
    sent(xrp, snd.at[13])
    sent(xrr, snd.at[9])
    sent(xro, snd.at[6])
    sent(zrq, snd.at[7])
    sent(zro, snd.at[8])
    sent(yrp, snd.at[11])
    gather_do.whole()
    gather_dq.whole()
    gather_do.done()
    gather_dq.done()


def finish(X, QB, OB, WG, DO, DQ, qw, ow, qm, qs, om, os_, *refs):
    (q_step, qw_new, q_copy, o_step, ow_new, o_copy, qm_out, qs_out, om_out, os_out,
     qstep, ostep, qnew, onew, qfull, ofull, vqc, voc, sem) = refs
    fs = lax.axis_index("z") * X + lax.axis_index("x")
    q_cols, o_cols = qm.shape[1], om.shape[1]
    q_rows, o_rows = qw.shape[0], ow.shape[0]
    blocks = QB.shape[0] * QB.shape[1]
    half_rank = QB.shape[4]
    puts = []

    def local(src, dst, number):
        copy = pltpu.make_async_copy(src, dst, sem.at[number])
        copy.start()
        return copy

    for number, (src, dst) in enumerate(((qm, qm_out), (qs, qs_out), (om, om_out), (os_, os_out))):
        puts.append(local(src, dst, 6 + number))

    def product(B, D):
        directions = D[...].reshape(2 * half_rank, -1)
        return sum(
            dot(B[:, :, half].reshape(-1, half_rank), directions[half * half_rank : (half + 1) * half_rank])
            for half in range(2)
        )

    full = product(QB, DQ)
    qfull[...] = full
    scale = lax.rsqrt(jnp.sum(full * full, axis=0, keepdims=True) / (blocks * q_rows) + 0.05)
    vqc[...] = (
        WG[:, :, 0:q_rows].reshape(blocks, q_rows, q_cols).astype(F32)
        - 0.01 * (qfull[...] * scale).reshape(blocks, q_rows, q_cols)
    ).astype(BF16).reshape(blocks * q_rows, q_cols)
    puts.append(local(vqc, q_copy, 0))
    step = qfull[pl.ds(pl.multiple_of(fs * q_rows, q_rows), q_rows), :] * scale
    qstep[...] = step
    qnew[...] = qw[...] - 0.01 * step
    puts.append(local(qstep, q_step, 1))
    puts.append(local(qnew, qw_new, 2))
    full = product(OB, DO)
    ofull[...] = full
    scale = lax.rsqrt(jnp.sum(full * full, axis=0, keepdims=True) / (blocks * o_rows) + 0.05)
    for half in range(o_cols // q_cols):
        part = slice(half * q_cols, (half + 1) * q_cols)
        rows = slice(q_rows + half * o_rows, q_rows + (half + 1) * o_rows)
        voc[:, part] = (
            WG[:, :, rows].reshape(blocks, o_rows, q_cols).astype(F32)
            - 0.01 * (ofull[:, part] * scale[:, part]).reshape(blocks, o_rows, q_cols)
        ).astype(BF16).reshape(blocks * o_rows, q_cols)
    puts.append(local(voc, o_copy, 3))
    step = ofull[pl.ds(pl.multiple_of(fs * o_rows, o_rows), o_rows), :] * scale
    ostep[...] = step
    onew[...] = ow[...] - 0.01 * step
    puts.append(local(ostep, o_step, 4))
    puts.append(local(onew, ow_new, 5))
    for copy in puts:
        copy.wait()


def shards(xin, qc, h, oc, qw, ow, qb, ob, qm, qs, om, os_):
    Z, X, Y, C = (lax.axis_size(name) for name in ("z", "x", "y", "c"))
    blocks = Z * X
    tokens, model = xin.shape
    rank = qb.shape[1]
    q_rows, o_rows, rank_rows = qw.shape[0], ow.shape[0], qm.shape[0]
    q_cols, o_cols = qw.shape[1], ow.shape[1]
    wide = h.shape[1]
    token_scale = (tokens * blocks * Y * C) ** (-0.5)
    halves = o_cols // q_cols
    w_rows = q_rows + halves * o_rows
    vmem = pl.BlockSpec(memory_space=pltpu.VMEM)
    any_spec = pl.BlockSpec(memory_space=pltpu.HBM)
    shape = jax.ShapeDtypeStruct
    qb_shape = (Z, X, 2, q_rows, rank // 2)
    ob_shape = (Z, X, 2, o_rows, rank // 2)
    wg_shape = (Z, X, w_rows, q_cols)
    do_shape = (Z, X, rank_rows, o_cols)
    dq_shape = (Z, X, rank_rows, q_cols)
    near_z = max(Z - 1, 1)
    part_x = (X, Z, rank_rows // 2, q_cols)
    part_y = (Y, Z, rank_rows // 2, q_cols)
    buffer = lambda *dims: pltpu.VMEM(dims, BF16)
    dma = lambda *dims: pltpu.SemaphoreType.DMA(dims)
    outs = pl.pallas_call(
        functools.partial(exchange, (Z, X, Y, token_scale)),
        out_shape=[
            pltpu.VMEM(qb_shape, BF16), pltpu.VMEM(ob_shape, BF16), pltpu.VMEM(wg_shape, BF16), pltpu.VMEM(do_shape, BF16),
            pltpu.VMEM(dq_shape, BF16),
            pltpu.VMEM(qm.shape, F32), pltpu.VMEM(qs.shape, F32), pltpu.VMEM(om.shape, F32), pltpu.VMEM(os_.shape, F32),
        ],
        in_specs=[any_spec] * 12,
        out_specs=[vmem] * 9,
        scratch_shapes=[
            buffer(tokens, model), buffer(tokens, wide), buffer(tokens, wide), buffer(tokens, model),
            buffer(2, rank // 2, tokens), buffer(2, rank // 2, tokens),
            pltpu.VMEM(qw.shape, F32), pltpu.VMEM(ow.shape, F32), pltpu.VMEM((tokens, rank // 2), F32),
            buffer(Y, rank, o_cols), buffer(Y, rank, o_cols), pltpu.VMEM((2, rank, o_cols), F32),
            buffer(Y, 2, rank // 2, o_cols), buffer(2, rank // 2, o_cols), buffer(2, 2, rank // 2, o_cols),
            buffer(X, Z, rank_rows, o_cols), buffer(X - 1, Z, rank_rows, o_cols),
            buffer(Z, rank_rows, o_cols), buffer(near_z, rank_rows, o_cols),
            buffer(Y, rank, q_cols), buffer(Y, rank, q_cols), pltpu.VMEM((Y, rank, q_cols), F32),
            buffer(X, *part_y), buffer(X - 1, *part_y), buffer(*part_y), buffer(Y - 1, *part_y[1:]),
            buffer(Y, *part_x), buffer(Y - 1, *part_x), buffer(*part_x), buffer(X - 1, *part_x[1:]),
            buffer(Z, rank_rows, q_cols), buffer(near_z, rank_rows, q_cols),
            dma(16), dma(15), dma(2, 4),
            dma(Z - 1), dma(Z, X - 1), dma(Z), dma(Z - 1), dma(Z, X - 1), dma(Z),
            dma(X - 1), dma(Z), dma(Z), dma(Z - 1), dma(Z - 1), dma(2, 2), dma(5),
            dma(Y), dma(2), dma(2, 2), dma(X - 1), dma(near_z), dma(Y), dma(X - 1), dma(Y - 1), dma(Y - 1), dma(X - 1), dma(near_z),
        ],
        compiler_params=pltpu.CompilerParams(collective_id=0, has_side_effects=True, vmem_limit_bytes=LIMIT),
        name="exchange",
    )(
        xin, qc, h, oc, qb, ob,
        qw, ow, qm, qs, om, os_,
    )
    qb_all, ob_all, wg_all, do_all, dq_all, qm_new, qs_new, om_new, os_new = outs
    (q_step, qw_new, q_copy, o_step, ow_new, o_copy, qm_new, qs_new, om_new, os_new) = pl.pallas_call(
        functools.partial(finish, X),
        out_shape=[
            shape(qw.shape, F32), shape(qw.shape, F32), shape((blocks * q_rows, q_cols), BF16),
            shape(ow.shape, F32), shape(ow.shape, F32), shape((blocks * o_rows, o_cols), BF16),
            shape(qm.shape, F32), shape(qs.shape, F32), shape(om.shape, F32), shape(os_.shape, F32),
        ],
        in_specs=[vmem] * 11,
        out_specs=[any_spec] * 10,
        scratch_shapes=[
            pltpu.VMEM(qw.shape, F32), pltpu.VMEM(ow.shape, F32), pltpu.VMEM(qw.shape, F32), pltpu.VMEM(ow.shape, F32),
            pltpu.VMEM((blocks * q_rows, q_cols), F32), pltpu.VMEM((blocks * o_rows, o_cols), F32),
            buffer(blocks * q_rows, q_cols), buffer(blocks * o_rows, o_cols),
            dma(10),
        ],
        compiler_params=pltpu.CompilerParams(vmem_limit_bytes=LIMIT // 2),
        name="finish",
    )(qb_all, ob_all, wg_all, do_all, dq_all, qw, ow, qm_new, qs_new, om_new, os_new)
    return (qm_new, qs_new, q_step, qw_new, q_copy, om_new, os_new, o_step, ow_new, o_copy)


def solution(mesh, split=(8, 4, 4, 2)):
    cube = Mesh(mesh.devices.reshape(split), FS_TP)
    tokens = P(FS_TP, None)
    tile = P(FS, TP)
    return jax.shard_map(
        shards,
        mesh=cube,
        in_specs=(tokens,) * 4 + (tile, tile, P(FS, None), P(FS, None)) + (tile,) * 4,
        out_specs=(tile, tile, tile, tile, P(None, TP), tile, tile, tile, tile, P(None, TP)),
        check_vma=False,
    )
```
